256 devices in a mesh: sp: 32 (over z, x), tp: 8 (over y, core).
Axes of the slice: x: 4, y: 4, z: 8, core: 2. Of those that a mesh axis runs over, the one named last changes fastest.
Arguments:
- layer_input: bfloat16 [16, 16384, 2048], P(None, ('sp', 'tp')), as said below
- key_weight: bfloat16 [2048, 384], replicated, may hold values from -0.125 to 0.125
- value_weight: bfloat16 [2048, 384], replicated, may hold values from -0.125 to 0.125
- queries: bfloat16 [96, 5, 64], P('sp'), may hold values from -6 to 6
- head_bias: float32 [6, 5], replicated, as said below
Outputs:
- stored: bfloat16 [96, 32, 512, 128], P('sp', None, 'tp')
- first_read: bfloat16 [96, 320], P('sp')
The draws below stay inside these ranges and needn't reach their ends.
Inputs may be any that keep to these rules, and one draw needn't show every extreme that they name: `layer_input`: entries lie between -12.5 and 12.5. `head_bias`: entries lie between -1 minus the natural logarithm of 16384 and -3.
All inputs are finite; a program needn't handle non-finite values.
Results may differ from the reference program's by a relative error of at most 0.01.
Values may be sent and summed in bfloat16 or wider, within the bound.
A program may use at most 64 MiB of HBM per device.

```python
import math
import jax
import jax.numpy as jnp
from jax import lax

D = 2048
HD = 64
KVH = 6
GROUP = 5
SUB = 64
SEQS = 16
PAIRS = 96
LEN = 16384
BLOCKS = 32
SPAN = 512


def draw_layer_input(key, part):
    base_key, scale_key = jax.random.split(key)
    blocks = LEN // SUB
    log_scale = jax.random.uniform(scale_key, (SEQS, blocks, 1, 1), jnp.float32, -0.7, 0.7)
    base = jnp.clip(jax.random.normal(base_key, (SEQS, blocks, SUB, D), jnp.float32), -6.0, 6.0)
    return (base * jnp.exp(log_scale)).reshape(SEQS, LEN, D).astype(jnp.bfloat16)


def draw_head_bias(key, part):
    kind_key, fast_key, slow_key = jax.random.split(key, 3)
    quick = jax.random.randint(kind_key, (KVH, GROUP), 0, 2) == 1
    fast = -math.log(40.0) + jax.random.uniform(fast_key, (KVH, GROUP), jnp.float32, -0.5, 0.5)
    slow = -math.log(LEN) - 0.5 + jax.random.uniform(slow_key, (KVH, GROUP), jnp.float32, -0.5, 0.5)
    return jnp.where(quick, fast, slow).astype(jnp.float32)


def shard_levels(rng, dims, cuts, least, top_value):
    def one(axis_at, parts):
        steps = jax.random.uniform(jax.random.fold_in(jax.random.fold_in(rng, 6), axis_at), (parts,), jnp.float32, least / len(cuts), top_value / len(cuts))
        return jnp.repeat(jnp.exp(steps), dims[axis_at] // parts).reshape((-1,) + (1,) * (len(dims) - axis_at - 1))

    level = one(*cuts[0])
    for cut in cuts[1:]:
        level = level * one(*cut)
    return level


def noise(own_key, dims, scale, most, cuts=(), held_as=jnp.bfloat16):
    factor_of = shard_levels(own_key, dims, cuts, -0.22, 0.18) if cuts else 1.0
    array = jax.random.normal(own_key, dims, jnp.float32) * scale * factor_of
    return jnp.minimum(jnp.maximum(array, -most), most).astype(held_as)


def setup_inputs(seed: int = 0) -> dict:
    streams_of = jax.random.split(jax.random.key(seed), 6)
    return {
        "layer_input": draw_layer_input(jax.random.fold_in(streams_of[5], 71), 0),
        "key_weight": noise(streams_of[1], (D, KVH * HD), D ** -0.5, 0.125),
        "value_weight": noise(streams_of[2], (D, KVH * HD), D ** -0.5, 0.125),
        "queries": noise(streams_of[3], (PAIRS, GROUP, HD), 1.0, 6.0, ((0, 32),)),
        "head_bias": draw_head_bias(jax.random.fold_in(streams_of[5], 71), 0),
    }


EPS_NORM = 0.0001

def reference(layer_input, key_weight, value_weight, queries, head_bias):
    tokens_flat = layer_input.reshape(SEQS * LEN, D)
    key_rows = jnp.dot(tokens_flat, key_weight, preferred_element_type=jnp.float32).astype(jnp.bfloat16).reshape(SEQS, LEN, KVH, HD)
    value_rows = jnp.dot(tokens_flat, value_weight, preferred_element_type=jnp.float32).astype(jnp.bfloat16).reshape(SEQS, LEN, KVH, HD)
    kv_rows = jnp.concatenate([key_rows, value_rows], axis=-1).transpose(0, 2, 1, 3).reshape(PAIRS, LEN, 2 * HD)
    head_shift = jnp.tile(head_bias, (SEQS, 1))
    score_scale = 1.0 / math.sqrt(HD)

    def read_pair(item):
        query, pair_rows, shift = item
        scores = jnp.dot(query, pair_rows[:, :HD].T, preferred_element_type=jnp.float32) * score_scale + shift[:, None]
        keep_log = jax.nn.log_sigmoid(-scores)
        suffix_log = lax.cumsum(keep_log, axis=1, reverse=True) - keep_log
        weights = jnp.exp(jax.nn.log_sigmoid(scores) + suffix_log).astype(jnp.bfloat16)
        return jnp.dot(weights, pair_rows[:, HD:], preferred_element_type=jnp.float32)
    summed = lax.map(read_pair, (queries, kv_rows, head_shift))
    squares = lax.optimization_barrier(jnp.mean(summed * summed, axis=-1, keepdims=True))
    first_read = (summed * lax.rsqrt(squares + EPS_NORM)).reshape(PAIRS, GROUP * HD).astype(jnp.bfloat16)
    return (kv_rows.reshape(PAIRS, BLOCKS, SPAN, 2 * HD), first_read)
```

```python
import functools

import jax
import jax.numpy as jnp
from jax import lax
from jax.experimental import pallas as pl
from jax.experimental.pallas import tpu as pltpu
from jax.sharding import PartitionSpec as P

HD = 64
KVH = 6
GROUP = 5
EPS_NORM = 0.0001
MESH = pl.DeviceIdType.MESH

NZ = 8
NX = 4
NSP = NZ * NX
NTP = 8
PAIRS = 3
ROWS = 64
LANES = 2 * HD
G8 = 8
R = PAIRS * G8
PLANE = NX * ROWS


def plane_offset(k):
    return jnp.where(k % 2 == 1, (k + 1) // 2, (NZ - k // 2) % NZ)


def split3(value):
    high = value.astype(jnp.bfloat16)
    rest = value - high.astype(jnp.float32)
    mid = rest.astype(jnp.bfloat16)
    low = (rest - mid.astype(jnp.float32)).astype(jnp.bfloat16)
    return high, mid, low


def exact_dot(value, ones):
    return sum(
        jnp.dot(part, ones, preferred_element_type=jnp.float32) for part in split3(value)
    )


def main_kernel(
    x_hbm, wk_hbm, wv_hbm, q_hbm, bias_hbm, land, usum,
    x_v, wk_v, wv_v, q_v, qp, bias_s, stage, vals, tots, part,
    x_sem, in_sem, send_sem, recv_sem, tot_in, part_in,
    tsend, trecv, psend, precv,
):
    sp = lax.axis_index("sp")
    tp = lax.axis_index("tp")
    z = sp // NX
    xm = sp % NX

    barrier = pltpu.get_barrier_semaphore()

    def greet_sp(i, c):
        pl.semaphore_signal(
            barrier, 1, device_id={"sp": (sp + i) % NSP}, device_id_type=MESH
        )
        return c

    lax.fori_loop(1, NSP, greet_sp, 0)
    for i in range(1, NTP):
        pl.semaphore_signal(
            barrier, 1, device_id={"tp": (tp + i) % NTP}, device_id_type=MESH
        )

    def x_copy(k):
        zt = (z + plane_offset(k)) % NZ
        return pltpu.make_async_copy(x_hbm.at[pl.ds(2 * zt, 2)], x_v.at[k], x_sem.at[k])

    wk_copy = pltpu.make_async_copy(wk_hbm, wk_v, in_sem.at[0])
    wv_copy = pltpu.make_async_copy(wv_hbm, wv_v, in_sem.at[1])
    q_copy = pltpu.make_async_copy(q_hbm, q_v, in_sem.at[2])
    bias_copy = pltpu.make_async_copy(bias_hbm, bias_s, in_sem.at[3])
    wk_copy.start()
    x_copy(0).start()
    wv_copy.start()
    for k in range(1, NZ):
        x_copy(k).start()
    q_copy.start()
    bias_copy.start()

    def block_copy(k, xt):
        zt = (z + plane_offset(k)) % NZ
        return pltpu.make_async_remote_copy(
            src_ref=stage.at[k, xt],
            dst_ref=land.at[:, sp],
            send_sem=send_sem.at[k, xt],
            recv_sem=recv_sem.at[k, xm],
            device_id={"sp": zt * NX + xt},
            device_id_type=MESH,
        )

    wk_copy.wait()
    wv_copy.wait()
    lane = lax.broadcasted_iota(jnp.int32, (ROWS, LANES), 1)
    low_half = lane < HD

    def project(k, c):
        x_copy(k).wait()
        x = x_v[k].reshape(2 * ROWS, x_v.shape[-1])
        keys = jnp.dot(x, wk_v[...], preferred_element_type=jnp.float32)
        values = jnp.dot(x, wv_v[...], preferred_element_type=jnp.float32)
        for half in range(2):
            for pair in range(3):
                kk = keys[half * ROWS : (half + 1) * ROWS, pair * LANES : (pair + 1) * LANES]
                vv = values[half * ROWS : (half + 1) * ROWS, pair * LANES : (pair + 1) * LANES]
                even = jnp.where(low_half, kk, pltpu.roll(vv, HD, 1))
                odd = jnp.where(low_half, pltpu.roll(kk, HD, 1), vv)
                for side, rows in ((0, even), (1, odd)):
                    head = 2 * pair + side
                    stage[k, 2 * half + head // 3, head % 3] = rows.astype(jnp.bfloat16)

        @pl.when(k == 0)
        def _():
            pl.semaphore_wait(barrier, NSP - 1 + NTP - 1)

        for xt in range(NX):
            @pl.when(jnp.logical_or(k > 0, xt != xm))
            def _():
                block_copy(k, xt).start()

        return c

    lax.fori_loop(0, NZ, project, 0)

    q_copy.wait()
    bias_copy.wait()
    qp[...] = jnp.zeros_like(qp)
    for p in range(PAIRS):
        for g in range(GROUP):
            qp[p, g : g + 1, 0:HD] = q_v[g, p : p + 1, :]
    row = lax.broadcasted_iota(jnp.int32, (R, PLANE), 0)
    bias = jnp.zeros((R, PLANE), jnp.float32)
    for p in range(PAIRS):
        head = (sp * PAIRS + p) % KVH
        for g in range(GROUP):
            bias = jnp.where(row == p * G8 + g, bias_s[head, g], bias)

    for xt in range(NX):
        @pl.when(xt == xm)
        def _():
            land[:, sp] = stage[0, xt]

    pos_i = lax.broadcasted_iota(jnp.int32, (PLANE, PLANE), 0)
    pos_j = lax.broadcasted_iota(jnp.int32, (PLANE, PLANE), 1)
    later = jnp.logical_and(pos_i > pos_j, pos_i // ROWS == pos_j // ROWS)
    later = jnp.where(later, 1.0, 0.0).astype(jnp.bfloat16)
    blk_i = lax.broadcasted_iota(jnp.int32, (PLANE, LANES), 0) // ROWS
    blk_j = lax.broadcasted_iota(jnp.int32, (PLANE, LANES), 1)
    lane_blk = lax.broadcasted_iota(jnp.int32, (G8, PLANE), 1) // ROWS

    def read_plane(k, total):
        zs = (z - plane_offset(k) + NZ) % NZ
        for xs in range(NX):
            @pl.when(jnp.logical_or(k > 0, xs != xm))
            def _():
                pltpu.make_async_remote_copy(
                    src_ref=stage.at[k, xs],
                    dst_ref=land.at[:, zs * NX + xs],
                    send_sem=send_sem.at[k, xs],
                    recv_sem=recv_sem.at[k, xs],
                    device_id={"sp": zs * NX + xs},
                    device_id_type=MESH,
                ).wait_recv()
        rows = [land[p, pl.ds(zs * NX, NX)].reshape(PLANE, LANES) for p in range(PAIRS)]
        scores = jnp.concatenate(
            [
                lax.dot_general(
                    qp[p], rows[p], (((1,), (1,)), ((), ())), preferred_element_type=jnp.float32
                )[:G8]
                for p in range(PAIRS)
            ],
            axis=0,
        )
        scores = scores * (1.0 / 8.0) + bias
        keep = -(jnp.maximum(scores, 0.0) + jnp.log1p(jnp.exp(-jnp.abs(scores))))
        inside = exact_dot(keep, later)
        pick = jnp.where(blk_i + zs * NX == blk_j, 1.0, 0.0).astype(jnp.bfloat16)
        total = total + exact_dot(keep, pick)
        weights = jnp.exp(scores + keep + inside)
        for p in range(PAIRS):
            w = weights[p * G8 : (p + 1) * G8]
            spread = jnp.concatenate(
                [jnp.where(lane_blk == b, w, 0.0) for b in range(NX)], axis=0
            ).astype(jnp.bfloat16)
            out = jnp.dot(spread, rows[p], preferred_element_type=jnp.float32)
            for b in range(NX):
                vals[zs * NX + b, p * G8 : (p + 1) * G8, :] = out[b * G8 : (b + 1) * G8]
        return total

    total = lax.fori_loop(0, NZ, read_plane, jnp.zeros((R, LANES), jnp.float32))

    def exchange(src, dst, ssem, rsem):
        for i in range(1, NTP):
            pltpu.make_async_remote_copy(
                src_ref=src, dst_ref=dst.at[i], send_sem=ssem.at[i], recv_sem=rsem.at[i],
                device_id={"tp": (tp + i) % NTP}, device_id_type=MESH,
            ).start()

    def arrived(src, dst, ssem, rsem):
        for i in range(1, NTP):
            pltpu.make_async_remote_copy(
                src_ref=src, dst_ref=dst.at[i], send_sem=ssem.at[i], recv_sem=rsem.at[i],
                device_id={"tp": (tp + i) % NTP}, device_id_type=MESH,
            ).wait()

    tots[...] = total
    exchange(tots, tot_in, tsend, trecv)
    arrived(tots, tot_in, tsend, trecv)
    every = total
    inside_later = jnp.zeros_like(total)
    for i in range(1, NTP):
        other = tot_in[i]
        every = every + other
        inside_later = inside_later + jnp.where(tp - i < 0, other, 0.0)
    chunk_i = lax.broadcasted_iota(jnp.int32, (LANES, LANES), 0)
    chunk_j = lax.broadcasted_iota(jnp.int32, (LANES, LANES), 1)
    after = jnp.where(chunk_i > chunk_j, 1.0, 0.0).astype(jnp.bfloat16)
    scale = jnp.exp(exact_dot(every, after) + inside_later)
    partial = jnp.zeros((R, LANES), jnp.float32)
    for b in range(NSP):
        partial = partial + scale[:, b : b + 1] * vals[b]
    part[...] = partial
    exchange(part, part_in, psend, precv)

    def drain(k, c):
        for xt in range(NX):
            @pl.when(jnp.logical_or(k > 0, xt != xm))
            def _():
                block_copy(k, xt).wait_send()
        return c

    lax.fori_loop(0, NZ, drain, 0)
    arrived(part, part_in, psend, precv)
    for i in range(1, NTP):
        partial = partial + part_in[i]
    usum[...] = partial


def finish_kernel(land, usum, stored, first_read, fr_v, out_sem):
    copy = pltpu.make_async_copy(land, stored, out_sem.at[0])
    copy.start()
    summed = usum[...]
    lane = lax.broadcasted_iota(jnp.int32, (R, LANES), 1)
    summed = jnp.where(lane >= HD, summed, 0.0)
    squares = jnp.sum(summed * summed, axis=-1, keepdims=True) * (1.0 / HD)
    normed = summed * lax.rsqrt(squares + EPS_NORM)
    swapped = pltpu.roll(normed, HD, 1)
    for p in range(PAIRS):
        for g in range(GROUP):
            source = normed if g % 2 else swapped
            lo = (g % 2) * HD
            fr_v[p : p + 1, g * HD : (g + 1) * HD] = source[
                p * G8 + g : p * G8 + g + 1, lo : lo + HD
            ]
    first_read[...] = fr_v[...].astype(jnp.bfloat16)
    copy.wait()


def per_device(layer_input, key_weight, value_weight, queries, head_bias):
    width = layer_input.shape[-1]
    hbm = pl.BlockSpec(memory_space=pltpu.HBM)
    vmem = pl.BlockSpec(memory_space=pltpu.VMEM)
    land, usum = pl.pallas_call(
        main_kernel,
        out_shape=(
            jax.ShapeDtypeStruct((PAIRS, NSP, ROWS, LANES), jnp.bfloat16),
            jax.ShapeDtypeStruct((R, LANES), jnp.float32),
        ),
        in_specs=[hbm] * 5,
        out_specs=(vmem, vmem),
        scratch_shapes=[
            pltpu.VMEM((NZ, 2, ROWS, width), jnp.bfloat16),
            pltpu.VMEM(key_weight.shape, jnp.bfloat16),
            pltpu.VMEM(value_weight.shape, jnp.bfloat16),
            pltpu.VMEM((GROUP, PAIRS, HD), jnp.bfloat16),
            pltpu.VMEM((PAIRS, 16, LANES), jnp.bfloat16),
            pltpu.SMEM(head_bias.shape, jnp.float32),
            pltpu.VMEM((NZ, NX, PAIRS, ROWS, LANES), jnp.bfloat16),
            pltpu.VMEM((NSP, R, LANES), jnp.float32),
            pltpu.VMEM((R, LANES), jnp.float32),
            pltpu.VMEM((R, LANES), jnp.float32),
            pltpu.SemaphoreType.DMA((NZ,)),
            pltpu.SemaphoreType.DMA((4,)),
            pltpu.SemaphoreType.DMA((NZ, NX)),
            pltpu.SemaphoreType.DMA((NZ, NX)),
            pltpu.VMEM((NTP, R, LANES), jnp.float32),
            pltpu.VMEM((NTP, R, LANES), jnp.float32),
            pltpu.SemaphoreType.DMA((NTP,)),
            pltpu.SemaphoreType.DMA((NTP,)),
            pltpu.SemaphoreType.DMA((NTP,)),
            pltpu.SemaphoreType.DMA((NTP,)),
        ],
        compiler_params=pltpu.CompilerParams(
            collective_id=0, has_side_effects=True, vmem_limit_bytes=53672 * 1024
        ),
        name="project_exchange_read",
    )(layer_input, key_weight, value_weight, queries.transpose(1, 0, 2), head_bias)
    stored, first_read = pl.pallas_call(
        finish_kernel,
        out_shape=(
            jax.ShapeDtypeStruct(land.shape, jnp.bfloat16),
            jax.ShapeDtypeStruct((PAIRS, GROUP * HD), jnp.bfloat16),
        ),
        in_specs=[pl.BlockSpec(memory_space=pl.ANY), vmem],
        out_specs=(pl.BlockSpec(memory_space=pl.ANY), vmem),
        scratch_shapes=[
            pltpu.VMEM((PAIRS, GROUP * HD), jnp.float32),
            pltpu.SemaphoreType.DMA((1,)),
        ],
        compiler_params=pltpu.CompilerParams(vmem_limit_bytes=8 * 1024 * 1024),
        name="finish",
    )(land, usum)
    return stored, first_read


def solution(mesh):
    in_specs = (P(None, ("sp", "tp"), None), P(), P(), P("sp", None, None), P())
    out_specs = (P("sp", None, "tp", None), P("sp", None))
    return jax.shard_map(
        per_device, mesh=mesh, in_specs=in_specs, out_specs=out_specs, check_vma=False
    )
```

```python
import functools

import jax
import jax.numpy as jnp
from jax import lax
from jax.experimental import pallas as pl
from jax.experimental.pallas import tpu as pltpu
from jax.sharding import PartitionSpec as P

HD = 64
KVH = 6
GROUP = 5
EPS_NORM = 0.0001
MESH = pl.DeviceIdType.MESH

NZ = 8
NX = 4
NSP = NZ * NX
NTP = 8
PAIRS = 3
ROWS = 64
LANES = 2 * HD
R = 16
PLANE = NX * ROWS
ORDER = (1, 7, 0, 2, 6, 3, 5, 4)
OWN = ORDER.index(0)
LAST = NZ - 1
FIRST_READS = 3


def plane_offset(k):
    offset = ORDER[-1]
    for at, value in enumerate(ORDER[:-1]):
        offset = jnp.where(k == at, value, offset)
    return offset


def split3(value):
    high = value.astype(jnp.bfloat16)
    rest = value - high.astype(jnp.float32)
    mid = rest.astype(jnp.bfloat16)
    low = (rest - mid.astype(jnp.float32)).astype(jnp.bfloat16)
    return high, mid, low


def exact_dot(value, ones):
    return sum(
        jnp.dot(part, ones, preferred_element_type=jnp.float32) for part in split3(value)
    )


def main_kernel(
    x_hbm, wk_hbm, wv_hbm, q_hbm, bias_hbm, land, usum,
    x_v, wk_v, wv_v, q_v, qc, bias_s, stage, vals, tots, part, tot_in, part_in,
    q_in, tv_out, tv_in,
    x_sem, in_sem, send_sem, recv_sem, tsend, trecv, psend, precv,
    qsend, qrecv, vsend, vrecv,
):
    sp = lax.axis_index("sp")
    tp = lax.axis_index("tp")
    z = sp // NX
    xm = sp % NX

    barrier = pltpu.get_barrier_semaphore()
    for i in range(1, NSP):
        pl.semaphore_signal(
            barrier, 1, device_id={"sp": (sp + i) % NSP}, device_id_type=MESH
        )
    for i in range(1, NTP):
        pl.semaphore_signal(
            barrier, 1, device_id={"tp": (tp + i) % NTP}, device_id_type=MESH
        )

    def x_copy(k):
        zt = (z + plane_offset(k)) % NZ
        return pltpu.make_async_copy(x_hbm.at[pl.ds(2 * zt, 2)], x_v.at[k], x_sem.at[k])

    wk_copy = pltpu.make_async_copy(wk_hbm, wk_v, in_sem.at[0])
    wv_copy = pltpu.make_async_copy(wv_hbm, wv_v, in_sem.at[1])
    q_copy = pltpu.make_async_copy(q_hbm, q_v, in_sem.at[2])
    bias_copy = pltpu.make_async_copy(bias_hbm, bias_s, in_sem.at[3])
    wk_copy.start()
    x_copy(0).start()
    wv_copy.start()
    for k in range(1, NZ):
        x_copy(k).start()
    q_copy.start()
    bias_copy.start()

    def block_copy(k, xt):
        zt = (z + plane_offset(k)) % NZ
        return pltpu.make_async_remote_copy(
            src_ref=stage.at[k, xt],
            dst_ref=land.at[:, sp],
            send_sem=send_sem.at[k, xt],
            recv_sem=recv_sem.at[k, xm],
            device_id={"sp": zt * NX + xt},
            device_id_type=MESH,
        )

    def send_plane(k):
        for dx in (1, 3, 2, 0):
            @pl.when(jnp.logical_or(k != OWN, dx != 0))
            def _():
                block_copy(k, (xm + dx) % NX).start()

    row_pair = lax.broadcasted_iota(jnp.int32, (R, PLANE), 0) // GROUP
    row_pair_v = lax.broadcasted_iota(jnp.int32, (NX * R, LANES), 0) % R // GROUP
    lane_blk = lax.broadcasted_iota(jnp.int32, (R, PLANE), 1) // ROWS
    pos_i = lax.broadcasted_iota(jnp.int32, (PLANE, PLANE), 0)
    pos_j = lax.broadcasted_iota(jnp.int32, (PLANE, PLANE), 1)
    later = jnp.logical_and(pos_i > pos_j, pos_i // ROWS == pos_j // ROWS)
    later = jnp.where(later, 1.0, 0.0).astype(jnp.bfloat16)
    blk_i = lax.broadcasted_iota(jnp.int32, (PLANE, LANES), 0) // ROWS
    blk_j = lax.broadcasted_iota(jnp.int32, (PLANE, LANES), 1)
    lane = lax.broadcasted_iota(jnp.int32, (R, LANES), 1)

    def bias_table(odd):
        row = lax.broadcasted_iota(jnp.int32, (R, PLANE), 0)
        table = jnp.zeros((R, PLANE), jnp.float32)
        for p in range(PAIRS):
            for g in range(GROUP):
                value = jnp.where(odd, bias_s[PAIRS + p, g], bias_s[p, g])
                table = jnp.where(row == p * GROUP + g, value, table)
        return table

    def read(rows, query, bias, first):
        scores = jnp.zeros((R, PLANE), jnp.float32)
        for p in range(PAIRS):
            dots = lax.dot_general(
                query, rows[p], (((1,), (1,)), ((), ())), preferred_element_type=jnp.float32
            )
            if dots.shape[0] == R:
                scores = jnp.where(row_pair == p, dots, scores)
            else:
                for b in range(NX):
                    mine = jnp.logical_and(row_pair == p, lane_blk == b)
                    scores = jnp.where(mine, dots[b * R : (b + 1) * R], scores)
        scores = scores * (1.0 / 8.0) + bias
        keep = -(jnp.maximum(scores, 0.0) + jnp.log1p(jnp.exp(-jnp.abs(scores))))
        inside = exact_dot(keep, later)
        pick = jnp.where(blk_i + first == blk_j, 1.0, 0.0).astype(jnp.bfloat16)
        totals = exact_dot(keep, pick)
        weights = jnp.exp(scores + keep + inside)
        spread = jnp.concatenate(
            [jnp.where(lane_blk == b, weights, 0.0) for b in range(NX)], axis=0
        ).astype(jnp.bfloat16)
        values = jnp.zeros((NX * R, LANES), jnp.float32)
        for p in range(PAIRS):
            out = jnp.dot(spread, rows[p], preferred_element_type=jnp.float32)
            values = jnp.where(row_pair_v == p, out, values)
        return totals, values

    q_copy.wait()
    bias_copy.wait()
    qc[...] = jnp.zeros_like(qc)
    for p in range(PAIRS):
        for g in range(GROUP):
            qc[p * GROUP + g : p * GROUP + g + 1, 0:HD] = q_v[g, p : p + 1, :]

    far = (z + NZ // 2) % NZ

    def query_copy(xt, slot):
        return pltpu.make_async_remote_copy(
            src_ref=qc, dst_ref=q_in.at[slot], send_sem=qsend.at[xt], recv_sem=qrecv.at[slot],
            device_id={"sp": far * NX + xt}, device_id_type=MESH,
        )

    def read_copy(xt, slot):
        return pltpu.make_async_remote_copy(
            src_ref=tv_out.at[xt], dst_ref=tv_in.at[slot],
            send_sem=vsend.at[xt], recv_sem=vrecv.at[slot],
            device_id={"sp": far * NX + xt}, device_id_type=MESH,
        )

    def read_at_source():
        for xt in range(NX):
            query_copy(xt, xt).wait_recv()
        rows = [stage[LAST, :, p].reshape(PLANE, LANES) for p in range(PAIRS)]
        totals, values = read(
            rows, q_in[...].reshape(NX * R, LANES), bias_table(lane_blk % 2 == 1), 0
        )
        for xt in range(NX):
            message = values[xt * R : (xt + 1) * R]
            for at, piece in enumerate(split3(totals[:, xt : xt + 1])):
                message = jnp.where(lane == at, piece.astype(jnp.float32), message)
            tv_out[xt] = message.astype(jnp.bfloat16)
        for dx in (1, 3, 2, 0):
            read_copy((xm + dx) % NX, xm).start()

    wk_copy.wait()
    wv_copy.wait()
    low_half = lax.broadcasted_iota(jnp.int32, (ROWS, LANES), 1) < HD

    def project(k, c):
        x_copy(k).wait()
        x = x_v[k].reshape(2 * ROWS, x_v.shape[-1])
        keys = jnp.dot(x, wk_v[...], preferred_element_type=jnp.float32)
        values = jnp.dot(x, wv_v[...], preferred_element_type=jnp.float32)
        for half in range(2):
            for pair in range(3):
                kk = keys[half * ROWS : (half + 1) * ROWS, pair * LANES : (pair + 1) * LANES]
                vv = values[half * ROWS : (half + 1) * ROWS, pair * LANES : (pair + 1) * LANES]
                even = jnp.where(low_half, kk, pltpu.roll(vv, HD, 1))
                odd = jnp.where(low_half, pltpu.roll(kk, HD, 1), vv)
                for side, rows in ((0, even), (1, odd)):
                    head = 2 * pair + side
                    stage[k, 2 * half + head // 3, head % 3] = rows.astype(jnp.bfloat16)

        @pl.when(k == 0)
        def _():
            pl.semaphore_wait(barrier, NSP - 1 + NTP - 1)
            for dx in range(NX):
                query_copy((xm + dx) % NX, xm).start()

        @pl.when(k != LAST)
        def _():
            send_plane(k)

        return c

    lax.fori_loop(0, NZ, project, 0)

    for xt in range(NX):
        @pl.when(xt == xm)
        def _():
            land[:, sp] = stage[OWN, xt]

    own_bias = bias_table(sp % 2 == 1)

    def arrival(k, xs):
        zs = (z - plane_offset(k) + NZ) % NZ
        return pltpu.make_async_remote_copy(
            src_ref=stage.at[k, xs],
            dst_ref=land.at[:, zs * NX + xs],
            send_sem=send_sem.at[k, xs],
            recv_sem=recv_sem.at[k, xs],
            device_id={"sp": zs * NX + xs},
            device_id_type=MESH,
        )

    def read_plane(k, total):
        zs = (z - plane_offset(k) + NZ) % NZ
        for xs in range(NX):
            @pl.when(jnp.logical_or(k != OWN, xs != xm))
            def _():
                arrival(k, xs).wait_recv()
        rows = [land[p, pl.ds(zs * NX, NX)].reshape(PLANE, LANES) for p in range(PAIRS)]
        totals, values = read(rows, qc[...], own_bias, zs * NX)
        for b in range(NX):
            vals[zs * NX + b] = values[b * R : (b + 1) * R]
        return total + totals

    total = jnp.zeros((R, LANES), jnp.float32)
    total = lax.fori_loop(0, FIRST_READS, read_plane, total)
    read_at_source()
    send_plane(LAST)
    total = lax.fori_loop(FIRST_READS, LAST, read_plane, total)
    for xs in range(NX):
        read_copy(xs, xs).wait_recv()
        message = tv_in[xs].astype(jnp.float32)
        sums = message[:, 0:1] + message[:, 1:2] + message[:, 2:3]
        total = total + jnp.where(lane == far * NX + xs, sums, 0.0)
        vals[far * NX + xs] = message

    def exchange(src, dst, ssem, rsem):
        return [
            pltpu.make_async_remote_copy(
                src_ref=src, dst_ref=dst.at[i], send_sem=ssem.at[i], recv_sem=rsem.at[i],
                device_id={"tp": (tp + i) % NTP}, device_id_type=MESH,
            )
            for i in range(1, NTP)
        ]

    tots[...] = total
    copies = exchange(tots, tot_in, tsend, trecv)
    for copy in copies:
        copy.start()
    for copy in copies:
        copy.wait()
    every = total
    inside_later = jnp.zeros_like(total)
    for i in range(1, NTP):
        other = tot_in[i]
        every = every + other
        inside_later = inside_later + jnp.where(tp - i < 0, other, 0.0)
    chunk_i = lax.broadcasted_iota(jnp.int32, (LANES, LANES), 0)
    chunk_j = lax.broadcasted_iota(jnp.int32, (LANES, LANES), 1)
    after = jnp.where(chunk_i > chunk_j, 1.0, 0.0).astype(jnp.bfloat16)
    scale = jnp.exp(exact_dot(every, after) + inside_later)
    partial = jnp.zeros((R, LANES), jnp.float32)
    for b in range(NSP):
        partial = partial + scale[:, b : b + 1] * vals[b]
    part[...] = partial
    copies = exchange(part, part_in, psend, precv)
    for copy in copies:
        copy.start()
    for copy in copies:
        copy.wait()
    for i in range(1, NTP):
        partial = partial + part_in[i]
    usum[...] = partial

    for xs in range(NX):
        arrival(LAST, xs).wait_recv()

    def drain(k, c):
        for xt in range(NX):
            @pl.when(jnp.logical_or(k != OWN, xt != xm))
            def _():
                block_copy(k, xt).wait_send()
        return c

    lax.fori_loop(0, NZ, drain, 0)
    for xt in range(NX):
        query_copy(xt, xt).wait_send()
        read_copy(xt, xt).wait_send()


def finish_kernel(land, usum, stored, first_read, fr_v, out_sem):
    copy = pltpu.make_async_copy(land, stored, out_sem.at[0])
    copy.start()
    summed = usum[...]
    lane = lax.broadcasted_iota(jnp.int32, (R, LANES), 1)
    summed = jnp.where(lane >= HD, summed, 0.0)
    squares = jnp.sum(summed * summed, axis=-1, keepdims=True) * (1.0 / HD)
    normed = summed * lax.rsqrt(squares + EPS_NORM)
    swapped = pltpu.roll(normed, HD, 1)
    for p in range(PAIRS):
        for g in range(GROUP):
            source = normed if g % 2 else swapped
            lo = (g % 2) * HD
            fr_v[p : p + 1, g * HD : (g + 1) * HD] = source[
                p * GROUP + g : p * GROUP + g + 1, lo : lo + HD
            ]
    first_read[...] = fr_v[...].astype(jnp.bfloat16)
    copy.wait()


def per_device(layer_input, key_weight, value_weight, queries, head_bias):
    width = layer_input.shape[-1]
    hbm = pl.BlockSpec(memory_space=pltpu.HBM)
    vmem = pl.BlockSpec(memory_space=pltpu.VMEM)
    land, usum = pl.pallas_call(
        main_kernel,
        out_shape=(
            jax.ShapeDtypeStruct((PAIRS, NSP, ROWS, LANES), jnp.bfloat16),
            jax.ShapeDtypeStruct((R, LANES), jnp.float32),
        ),
        in_specs=[hbm] * 5,
        out_specs=(vmem, vmem),
        scratch_shapes=[
            pltpu.VMEM((NZ, 2, ROWS, width), jnp.bfloat16),
            pltpu.VMEM(key_weight.shape, jnp.bfloat16),
            pltpu.VMEM(value_weight.shape, jnp.bfloat16),
            pltpu.VMEM((GROUP, PAIRS, HD), jnp.bfloat16),
            pltpu.VMEM((R, LANES), jnp.bfloat16),
            pltpu.SMEM(head_bias.shape, jnp.float32),
            pltpu.VMEM((NZ, NX, PAIRS, ROWS, LANES), jnp.bfloat16),
            pltpu.VMEM((NSP, R, LANES), jnp.float32),
            pltpu.VMEM((R, LANES), jnp.float32),
            pltpu.VMEM((R, LANES), jnp.float32),
            pltpu.VMEM((NTP, R, LANES), jnp.float32),
            pltpu.VMEM((NTP, R, LANES), jnp.float32),
            pltpu.VMEM((NX, R, LANES), jnp.bfloat16),
            pltpu.VMEM((NX, R, LANES), jnp.bfloat16),
            pltpu.VMEM((NX, R, LANES), jnp.bfloat16),
            pltpu.SemaphoreType.DMA((NZ,)),
            pltpu.SemaphoreType.DMA((4,)),
            pltpu.SemaphoreType.DMA((NZ, NX)),
            pltpu.SemaphoreType.DMA((NZ, NX)),
            pltpu.SemaphoreType.DMA((NTP,)),
            pltpu.SemaphoreType.DMA((NTP,)),
            pltpu.SemaphoreType.DMA((NTP,)),
            pltpu.SemaphoreType.DMA((NTP,)),
            pltpu.SemaphoreType.DMA((NX,)),
            pltpu.SemaphoreType.DMA((NX,)),
            pltpu.SemaphoreType.DMA((NX,)),
            pltpu.SemaphoreType.DMA((NX,)),
        ],
        compiler_params=pltpu.CompilerParams(
            collective_id=0, has_side_effects=True, vmem_limit_bytes=53672 * 1024
        ),
        name="project_exchange_read",
    )(layer_input, key_weight, value_weight, queries.transpose(1, 0, 2), head_bias)
    stored, first_read = pl.pallas_call(
        finish_kernel,
        out_shape=(
            jax.ShapeDtypeStruct(land.shape, jnp.bfloat16),
            jax.ShapeDtypeStruct((PAIRS, GROUP * HD), jnp.bfloat16),
        ),
        in_specs=[pl.BlockSpec(memory_space=pl.ANY), vmem],
        out_specs=(pl.BlockSpec(memory_space=pl.ANY), vmem),
        scratch_shapes=[
            pltpu.VMEM((PAIRS, GROUP * HD), jnp.float32),
            pltpu.SemaphoreType.DMA((1,)),
        ],
        compiler_params=pltpu.CompilerParams(vmem_limit_bytes=8 * 1024 * 1024),
        name="finish",
    )(land, usum)
    return stored, first_read


def solution(mesh):
    in_specs = (P(None, ("sp", "tp"), None), P(), P(), P("sp", None, None), P())
    out_specs = (P("sp", None, "tp", None), P("sp", None))
    return jax.shard_map(
        per_device, mesh=mesh, in_specs=in_specs, out_specs=out_specs, check_vma=False
    )
```

```python
import functools

import jax
import jax.numpy as jnp
from jax import lax
from jax.experimental import pallas as pl
from jax.experimental.pallas import tpu as pltpu
from jax.sharding import PartitionSpec as P

HD = 64
KVH = 6
GROUP = 5
EPS_NORM = 0.0001
MESH = pl.DeviceIdType.MESH

NZ = 8
NX = 4
NSP = NZ * NX
NTP = 8
PAIRS = 3
ROWS = 64
LANES = 2 * HD
R = 16
PLANE = NX * ROWS
CUTS = 4
ORDER = (1, 7, 0, 2, 6, 4, 3, 5)
OWN = ORDER.index(0)
LAST = ORDER.index(NZ // 2)


def plane_offset(k):
    offset = ORDER[-1]
    for at, value in enumerate(ORDER[:-1]):
        offset = jnp.where(k == at, value, offset)
    return offset


def split3(value):
    high = value.astype(jnp.bfloat16)
    rest = value - high.astype(jnp.float32)
    mid = rest.astype(jnp.bfloat16)
    low = (rest - mid.astype(jnp.float32)).astype(jnp.bfloat16)
    return high, mid, low


def exact_dot(value, ones):
    rows = value.shape[0]
    parts = jnp.concatenate(split3(value), axis=0)
    sums = jnp.dot(parts, ones, preferred_element_type=jnp.float32)
    return sums[:rows] + sums[rows : 2 * rows] + sums[2 * rows :]


def main_kernel(
    x_hbm, wk_hbm, wv_hbm, q_hbm, bias_hbm, land, usum,
    x_v, wk_v, wv_v, q_v, qc, bias_s, stage, vals, tots, part, tot_in, part_in,
    q_out, q_in, tv_out, tv_in,
    x_sem, w_sem, in_sem, send_sem, recv_sem, tsend, trecv, psend, precv,
    qsend, qrecv, vsend, vrecv,
):
    sp = lax.axis_index("sp")
    tp = lax.axis_index("tp")
    z = sp // NX
    xm = sp % NX

    def x_copy(k):
        zt = (z + plane_offset(k)) % NZ
        return pltpu.make_async_copy(x_hbm.at[pl.ds(2 * zt, 2)], x_v.at[k], x_sem.at[k])

    def weight_copies(w_hbm, w_v, first):
        part = w_v.shape[0] // CUTS
        return [
            pltpu.make_async_copy(
                w_hbm.at[pl.ds(i * part, part)], w_v.at[pl.ds(i * part, part)], w_sem.at[first + i]
            )
            for i in range(CUTS)
        ]

    weights = weight_copies(wk_hbm, wk_v, 0) + weight_copies(wv_hbm, wv_v, CUTS)
    q_copy = pltpu.make_async_copy(q_hbm, q_v, in_sem.at[0])
    bias_copy = pltpu.make_async_copy(bias_hbm, bias_s, in_sem.at[1])
    x_copy(0).start()
    for copy in weights:
        copy.start()
    q_copy.start()
    bias_copy.start()
    for k in range(1, NZ):
        x_copy(k).start()

    barrier = pltpu.get_barrier_semaphore()
    for i in range(1, NSP):
        pl.semaphore_signal(
            barrier, 1, device_id={"sp": (sp + i) % NSP}, device_id_type=MESH
        )
    for i in range(1, NTP):
        pl.semaphore_signal(
            barrier, 1, device_id={"tp": (tp + i) % NTP}, device_id_type=MESH
        )

    def block_copy(k, xt):
        zt = (z + plane_offset(k)) % NZ
        return pltpu.make_async_remote_copy(
            src_ref=stage.at[k, xt],
            dst_ref=land.at[:, sp],
            send_sem=send_sem.at[k, xt],
            recv_sem=recv_sem.at[k, xm],
            device_id={"sp": zt * NX + xt},
            device_id_type=MESH,
        )

    def send_plane(k):
        for dx in (1, 3, 2, 0):
            @pl.when(jnp.logical_or(k != OWN, dx != 0))
            def _():
                block_copy(k, (xm + dx) % NX).start()

    row_pair = lax.broadcasted_iota(jnp.int32, (R, PLANE), 0) // GROUP
    row_pair_v = lax.broadcasted_iota(jnp.int32, (NX * R, LANES), 0) % R // GROUP
    lane_blk = lax.broadcasted_iota(jnp.int32, (R, PLANE), 1) // ROWS
    pos_i = lax.broadcasted_iota(jnp.int32, (PLANE, PLANE), 0)
    pos_j = lax.broadcasted_iota(jnp.int32, (PLANE, PLANE), 1)
    later = jnp.logical_and(pos_i > pos_j, pos_i // ROWS == pos_j // ROWS)
    later = jnp.where(later, 1.0, 0.0).astype(jnp.bfloat16)
    blk_i = lax.broadcasted_iota(jnp.int32, (PLANE, LANES), 0) // ROWS
    blk_j = lax.broadcasted_iota(jnp.int32, (PLANE, LANES), 1)
    lane = lax.broadcasted_iota(jnp.int32, (R, LANES), 1)

    def bias_table(odd):
        row = lax.broadcasted_iota(jnp.int32, (R, PLANE), 0)
        table = jnp.zeros((R, PLANE), jnp.float32)
        for p in range(PAIRS):
            for g in range(GROUP):
                value = jnp.where(odd, bias_s[PAIRS + p, g], bias_s[p, g])
                table = jnp.where(row == p * GROUP + g, value, table)
        return table

    def read(rows, query, bias, first):
        scores = jnp.zeros((R, PLANE), jnp.float32)
        for p in range(PAIRS):
            dots = lax.dot_general(
                query, rows[p], (((1,), (1,)), ((), ())), preferred_element_type=jnp.float32
            )
            if dots.shape[0] == R:
                scores = jnp.where(row_pair == p, dots, scores)
            else:
                for b in range(NX):
                    mine = jnp.logical_and(row_pair == p, lane_blk == b)
                    scores = jnp.where(mine, dots[b * R : (b + 1) * R], scores)
        scores = scores * (1.0 / 8.0) + bias
        keep = -(jnp.maximum(scores, 0.0) + jnp.log1p(jnp.exp(-jnp.abs(scores))))
        pick = jnp.where(blk_i + first == blk_j, 1.0, 0.0).astype(jnp.bfloat16)
        sums = exact_dot(keep, jnp.concatenate([later, pick], axis=1))
        inside, totals = sums[:, :PLANE], sums[:, PLANE:]
        weights = jnp.exp(scores + keep + inside)
        spread = jnp.concatenate(
            [jnp.where(lane_blk == b, weights, 0.0) for b in range(NX)], axis=0
        ).astype(jnp.bfloat16)
        values = jnp.zeros((NX * R, LANES), jnp.float32)
        for p in range(PAIRS):
            out = jnp.dot(spread, rows[p], preferred_element_type=jnp.float32)
            values = jnp.where(row_pair_v == p, out, values)
        return totals, values

    q_copy.wait()
    bias_copy.wait()
    qc[...] = jnp.zeros_like(qc)
    for p in range(PAIRS):
        for g in range(GROUP):
            qc[p * GROUP + g : p * GROUP + g + 1, 0:HD] = q_v[g, p : p + 1, :]
    wide = qc[...].astype(jnp.float32)
    q_out[...] = (wide[: R // 2] + pltpu.roll(wide[R // 2 :], HD, 1)).astype(jnp.bfloat16)

    far = (z + NZ // 2) % NZ

    def query_copy(xt, slot):
        return pltpu.make_async_remote_copy(
            src_ref=q_out, dst_ref=q_in.at[slot], send_sem=qsend.at[xt], recv_sem=qrecv.at[slot],
            device_id={"sp": far * NX + xt}, device_id_type=MESH,
        )

    def read_copy(xt, slot):
        return pltpu.make_async_remote_copy(
            src_ref=tv_out.at[xt], dst_ref=tv_in.at[slot],
            send_sem=vsend.at[xt], recv_sem=vrecv.at[slot],
            device_id={"sp": far * NX + xt}, device_id_type=MESH,
        )

    def read_at_source():
        for xt in range(NX):
            query_copy(xt, xt).wait_recv()
        rows = [stage[LAST, :, p].reshape(PLANE, LANES) for p in range(PAIRS)]
        low = lane[: R // 2] < HD
        pieces = []
        for xt in range(NX):
            wide = q_in[xt].astype(jnp.float32)
            pieces += [jnp.where(low, wide, 0.0), jnp.where(low, pltpu.roll(wide, HD, 1), 0.0)]
        query = jnp.concatenate(pieces, axis=0).astype(jnp.bfloat16)
        totals, values = read(rows, query, bias_table(lane_blk % 2 == 1), 0)
        for xt in range(NX):
            message = values[xt * R : (xt + 1) * R]
            for at, piece in enumerate(split3(totals[:, xt : xt + 1])):
                message = jnp.where(lane == at, piece.astype(jnp.float32), message)
            tv_out[xt] = message.astype(jnp.bfloat16)
        for dx in (1, 3, 2, 0):
            read_copy((xm + dx) % NX, xm).start()

    for copy in weights:
        copy.wait()
    low_half = lax.broadcasted_iota(jnp.int32, (ROWS, LANES), 1) < HD

    def project(k, c):
        x_copy(k).wait()
        x = x_v[k].reshape(2 * ROWS, x_v.shape[-1])
        keys = jnp.dot(x, wk_v[...], preferred_element_type=jnp.float32)
        values = jnp.dot(x, wv_v[...], preferred_element_type=jnp.float32)
        for half in range(2):
            for pair in range(3):
                kk = keys[half * ROWS : (half + 1) * ROWS, pair * LANES : (pair + 1) * LANES]
                vv = values[half * ROWS : (half + 1) * ROWS, pair * LANES : (pair + 1) * LANES]
                even = jnp.where(low_half, kk, pltpu.roll(vv, HD, 1))
                odd = jnp.where(low_half, pltpu.roll(kk, HD, 1), vv)
                for side, rows in ((0, even), (1, odd)):
                    head = 2 * pair + side
                    stage[k, 2 * half + head // 3, head % 3] = rows.astype(jnp.bfloat16)

        @pl.when(k == 0)
        def _():
            pl.semaphore_wait(barrier, NSP - 1 + NTP - 1)
            for dx in range(NX):
                query_copy((xm + dx) % NX, xm).start()

        @pl.when(k == LAST)
        def _():
            read_at_source()

        @pl.when(k != LAST)
        def _():
            send_plane(k)

        return c

    lax.fori_loop(0, NZ, project, 0)
    send_plane(LAST)

    for xt in range(NX):
        @pl.when(xt == xm)
        def _():
            land[:, sp] = stage[OWN, xt]

    own_bias = bias_table(sp % 2 == 1)

    def arrival(k, xs):
        zs = (z - plane_offset(k) + NZ) % NZ
        return pltpu.make_async_remote_copy(
            src_ref=stage.at[k, xs],
            dst_ref=land.at[:, zs * NX + xs],
            send_sem=send_sem.at[k, xs],
            recv_sem=recv_sem.at[k, xs],
            device_id={"sp": zs * NX + xs},
            device_id_type=MESH,
        )

    def read_plane(at, c):
        k = at + jnp.where(at < LAST, 0, 1)
        zs = (z - plane_offset(k) + NZ) % NZ

        @pl.when(at == NZ - 2)
        def _():
            for xs in range(NX):
                read_copy(xs, xs).wait_recv()
                message = tv_in[xs].astype(jnp.float32)
                sums = message[:, 0:1] + message[:, 1:2] + message[:, 2:3]
                tots[...] += jnp.where(lane == far * NX + xs, sums, 0.0)
                vals[far * NX + xs] = message

        for xs in range(NX):
            @pl.when(jnp.logical_or(k != OWN, xs != xm))
            def _():
                arrival(k, xs).wait_recv()
        rows = [land[p, pl.ds(zs * NX, NX)].reshape(PLANE, LANES) for p in range(PAIRS)]
        totals, values = read(rows, qc[...], own_bias, zs * NX)
        tots[...] += totals
        for b in range(NX):
            vals[zs * NX + b] = values[b * R : (b + 1) * R]
        return c

    tots[...] = jnp.zeros((R, LANES), jnp.float32)
    lax.fori_loop(0, NZ - 1, read_plane, 0)

    def exchange(src, dst, ssem, rsem):
        return [
            pltpu.make_async_remote_copy(
                src_ref=src, dst_ref=dst.at[i], send_sem=ssem.at[i], recv_sem=rsem.at[i],
                device_id={"tp": (tp + i) % NTP}, device_id_type=MESH,
            )
            for i in range(1, NTP)
        ]

    copies = exchange(tots, tot_in, tsend, trecv)
    for copy in copies:
        copy.start()
    for copy in copies:
        copy.wait()
    every = tots[...]
    inside_later = jnp.zeros_like(every)
    for i in range(1, NTP):
        other = tot_in[i]
        every = every + other
        inside_later = inside_later + jnp.where(tp - i < 0, other, 0.0)
    chunk_i = lax.broadcasted_iota(jnp.int32, (LANES, LANES), 0)
    chunk_j = lax.broadcasted_iota(jnp.int32, (LANES, LANES), 1)
    after = jnp.where(chunk_i > chunk_j, 1.0, 0.0).astype(jnp.bfloat16)
    scale = jnp.exp(exact_dot(every, after) + inside_later)
    partial = jnp.zeros((R, LANES), jnp.float32)
    for b in range(NSP):
        partial = partial + scale[:, b : b + 1] * vals[b]
    part[...] = partial
    copies = exchange(part, part_in, psend, precv)
    for copy in copies:
        copy.start()

    for xs in range(NX):
        arrival(LAST, xs).wait_recv()

    def drain(k, c):
        for xt in range(NX):
            @pl.when(jnp.logical_or(k != OWN, xt != xm))
            def _():
                block_copy(k, xt).wait_send()
        return c

    lax.fori_loop(0, NZ, drain, 0)
    for xt in range(NX):
        query_copy(xt, xt).wait_send()
        read_copy(xt, xt).wait_send()

    for copy in copies:
        copy.wait()
    for i in range(1, NTP):
        partial = partial + part_in[i]
    usum[...] = partial


def finish_kernel(land, usum, stored, first_read, fr_v, fr_b, out_sem, fr_sem):
    copies = [
        pltpu.make_async_copy(
            land.at[p, pl.ds(half * NSP // 4, NSP // 4)],
            stored.at[p, pl.ds(half * NSP // 4, NSP // 4)],
            out_sem.at[p, half],
        )
        for p in range(PAIRS)
        for half in range(4)
    ]
    for copy in copies:
        copy.start()
    summed = usum[...]
    lane = lax.broadcasted_iota(jnp.int32, (R, LANES), 1)
    summed = jnp.where(lane >= HD, summed, 0.0)
    squares = jnp.sum(summed * summed, axis=-1, keepdims=True) * (1.0 / HD)
    normed = summed * lax.rsqrt(squares + EPS_NORM)
    swapped = pltpu.roll(normed, HD, 1)
    for p in range(PAIRS):
        for g in range(GROUP):
            source = normed if g % 2 else swapped
            lo = (g % 2) * HD
            fr_v[p : p + 1, g * HD : (g + 1) * HD] = source[
                p * GROUP + g : p * GROUP + g + 1, lo : lo + HD
            ]
    fr_b[...] = fr_v[...].astype(jnp.bfloat16)
    fr_copy = pltpu.make_async_copy(fr_b, first_read, fr_sem.at[0])
    fr_copy.start()
    for copy in copies:
        copy.wait()
    fr_copy.wait()


def per_device(layer_input, key_weight, value_weight, queries, head_bias):
    width = layer_input.shape[-1]
    hbm = pl.BlockSpec(memory_space=pltpu.HBM)
    vmem = pl.BlockSpec(memory_space=pltpu.VMEM)
    land, usum = pl.pallas_call(
        main_kernel,
        out_shape=(
            jax.ShapeDtypeStruct((PAIRS, NSP, ROWS, LANES), jnp.bfloat16),
            jax.ShapeDtypeStruct((R, LANES), jnp.float32),
        ),
        in_specs=[hbm] * 5,
        out_specs=(vmem, vmem),
        scratch_shapes=[
            pltpu.VMEM((NZ, 2, ROWS, width), jnp.bfloat16),
            pltpu.VMEM(key_weight.shape, jnp.bfloat16),
            pltpu.VMEM(value_weight.shape, jnp.bfloat16),
            pltpu.VMEM((GROUP, PAIRS, HD), jnp.bfloat16),
            pltpu.VMEM((R, LANES), jnp.bfloat16),
            pltpu.SMEM(head_bias.shape, jnp.float32),
            pltpu.VMEM((NZ, NX, PAIRS, ROWS, LANES), jnp.bfloat16),
            pltpu.VMEM((NSP, R, LANES), jnp.float32),
            pltpu.VMEM((R, LANES), jnp.float32),
            pltpu.VMEM((R, LANES), jnp.float32),
            pltpu.VMEM((NTP, R, LANES), jnp.float32),
            pltpu.VMEM((NTP, R, LANES), jnp.float32),
            pltpu.VMEM((R // 2, LANES), jnp.bfloat16),
            pltpu.VMEM((NX, R // 2, LANES), jnp.bfloat16),
            pltpu.VMEM((NX, R, LANES), jnp.bfloat16),
            pltpu.VMEM((NX, R, LANES), jnp.bfloat16),
            pltpu.SemaphoreType.DMA((NZ,)),
            pltpu.SemaphoreType.DMA((2 * CUTS,)),
            pltpu.SemaphoreType.DMA((2,)),
            pltpu.SemaphoreType.DMA((NZ, NX)),
            pltpu.SemaphoreType.DMA((NZ, NX)),
            pltpu.SemaphoreType.DMA((NTP,)),
            pltpu.SemaphoreType.DMA((NTP,)),
            pltpu.SemaphoreType.DMA((NTP,)),
            pltpu.SemaphoreType.DMA((NTP,)),
            pltpu.SemaphoreType.DMA((NX,)),
            pltpu.SemaphoreType.DMA((NX,)),
            pltpu.SemaphoreType.DMA((NX,)),
            pltpu.SemaphoreType.DMA((NX,)),
        ],
        compiler_params=pltpu.CompilerParams(
            collective_id=0, has_side_effects=True, vmem_limit_bytes=40 * 1024 * 1024
        ),
        name="project_exchange_read",
    )(
        *(
            pltpu.with_memory_space_constraint(operand, pltpu.HBM)
            for operand in (
                layer_input, key_weight, value_weight, queries.transpose(1, 0, 2), head_bias
            )
        )
    )
    stored, first_read = pl.pallas_call(
        finish_kernel,
        out_shape=(
            jax.ShapeDtypeStruct(land.shape, jnp.bfloat16),
            jax.ShapeDtypeStruct((PAIRS, GROUP * HD), jnp.bfloat16),
        ),
        in_specs=[pl.BlockSpec(memory_space=pl.ANY), vmem],
        out_specs=(pl.BlockSpec(memory_space=pl.ANY), pl.BlockSpec(memory_space=pl.ANY)),
        scratch_shapes=[
            pltpu.VMEM((PAIRS, GROUP * HD), jnp.float32),
            pltpu.VMEM((PAIRS, GROUP * HD), jnp.bfloat16),
            pltpu.SemaphoreType.DMA((PAIRS, 4)),
            pltpu.SemaphoreType.DMA((1,)),
        ],
        compiler_params=pltpu.CompilerParams(vmem_limit_bytes=8 * 1024 * 1024),
        name="finish",
    )(land, usum)
    return stored, first_read


def solution(mesh):
    in_specs = (P(None, ("sp", "tp"), None), P(), P(), P("sp", None, None), P())
    out_specs = (P("sp", None, "tp", None), P("sp", None))
    return jax.shard_map(
        per_device, mesh=mesh, in_specs=in_specs, out_specs=out_specs, check_vma=False
    )
```

```python
import functools

import jax
import jax.numpy as jnp
from jax import lax
from jax.experimental import pallas as pl
from jax.experimental.pallas import tpu as pltpu
from jax.sharding import PartitionSpec as P

HD = 64
KVH = 6
GROUP = 5
EPS_NORM = 0.0001
MESH = pl.DeviceIdType.MESH

NZ = 8
NX = 4
NSP = NZ * NX
NTP = 8
PAIRS = 3
ROWS = 64
LANES = 2 * HD
R = 16
PLANE = NX * ROWS
CUTS = 4
ORDER = (1, 7, 0, 2, 6, 4, 3, 5)
OWN = ORDER.index(0)
LAST = ORDER.index(NZ // 2)


def plane_offset(k):
    offset = ORDER[-1]
    for at, value in enumerate(ORDER[:-1]):
        offset = jnp.where(k == at, value, offset)
    return offset


def split3(value):
    high = value.astype(jnp.bfloat16)
    rest = value - high.astype(jnp.float32)
    mid = rest.astype(jnp.bfloat16)
    low = (rest - mid.astype(jnp.float32)).astype(jnp.bfloat16)
    return high, mid, low


def exact_dot(value, ones):
    rows = value.shape[0]
    parts = jnp.concatenate(split3(value), axis=0)
    sums = jnp.dot(parts, ones, preferred_element_type=jnp.float32)
    return sums[:rows] + sums[rows : 2 * rows] + sums[2 * rows :]


def main_kernel(
    x_hbm, wk_hbm, wv_hbm, q_hbm, bias_hbm, land, usum,
    x_v, wk_v, wv_v, q_v, qc, bias_s, stage, vals, tots, part, tot_in, part_in,
    q_out, q_in, tv_out, tv_in,
    x_sem, w_sem, in_sem, send_sem, recv_sem, tsend, trecv, psend, precv,
    qsend, qrecv, vsend, vrecv,
):
    sp = lax.axis_index("sp")
    tp = lax.axis_index("tp")
    z = sp // NX
    xm = sp % NX

    def x_copy(k):
        zt = (z + plane_offset(k)) % NZ
        return pltpu.make_async_copy(x_hbm.at[pl.ds(2 * zt, 2)], x_v.at[k], x_sem.at[k])

    def weight_copies(w_hbm, w_v, which):
        part = w_v.shape[0] // CUTS
        return [
            pltpu.make_async_copy(
                w_hbm.at[pl.ds(i * part, part)], w_v.at[pl.ds(i * part, part)], w_sem.at[which]
            )
            for i in range(CUTS)
        ]

    weights = weight_copies(wk_hbm, wk_v, 0) + weight_copies(wv_hbm, wv_v, 1)
    q_copy = pltpu.make_async_copy(q_hbm, q_v, in_sem.at[0])
    bias_copy = pltpu.make_async_copy(bias_hbm, bias_s, in_sem.at[1])
    x_copy(0).start()
    for copy in weights:
        copy.start()
    q_copy.start()
    bias_copy.start()
    for k in range(1, NZ):
        x_copy(k).start()

    barrier = pltpu.get_barrier_semaphore()
    for i in range(1, NSP):
        pl.semaphore_signal(
            barrier, 1, device_id={"sp": (sp + i) % NSP}, device_id_type=MESH
        )
    for i in range(1, NTP):
        pl.semaphore_signal(
            barrier, 1, device_id={"tp": (tp + i) % NTP}, device_id_type=MESH
        )

    def block_copy(k, xt):
        zt = (z + plane_offset(k)) % NZ
        return pltpu.make_async_remote_copy(
            src_ref=stage.at[k, xt],
            dst_ref=land.at[:, sp],
            send_sem=send_sem.at[k],
            recv_sem=recv_sem.at[k],
            device_id={"sp": zt * NX + xt},
            device_id_type=MESH,
        )

    def group(ref, ssem, rsem):
        return pltpu.make_async_remote_copy(
            src_ref=ref, dst_ref=ref, send_sem=ssem, recv_sem=rsem,
            device_id={"sp": sp}, device_id_type=MESH,
        )

    def send_plane(k):
        for dx in (1, 3, 2, 0):
            @pl.when(jnp.logical_or(k != OWN, dx != 0))
            def _():
                block_copy(k, (xm + dx) % NX).start()

    row_pair = lax.broadcasted_iota(jnp.int32, (R, PLANE), 0) // GROUP
    row_pair_v = lax.broadcasted_iota(jnp.int32, (NX * R, LANES), 0) % R // GROUP
    lane_blk = lax.broadcasted_iota(jnp.int32, (R, PLANE), 1) // ROWS
    pos_i = lax.broadcasted_iota(jnp.int32, (PLANE, PLANE), 0)
    pos_j = lax.broadcasted_iota(jnp.int32, (PLANE, PLANE), 1)
    later = jnp.logical_and(pos_i > pos_j, pos_i // ROWS == pos_j // ROWS)
    later = jnp.where(later, 1.0, 0.0).astype(jnp.bfloat16)
    blk_i = lax.broadcasted_iota(jnp.int32, (PLANE, LANES), 0) // ROWS
    blk_j = lax.broadcasted_iota(jnp.int32, (PLANE, LANES), 1)
    lane = lax.broadcasted_iota(jnp.int32, (R, LANES), 1)

    def bias_table(odd):
        row = lax.broadcasted_iota(jnp.int32, (R, PLANE), 0)
        table = jnp.zeros((R, PLANE), jnp.float32)
        for p in range(PAIRS):
            for g in range(GROUP):
                value = jnp.where(odd, bias_s[PAIRS + p, g], bias_s[p, g])
                table = jnp.where(row == p * GROUP + g, value, table)
        return table

    def read(rows, query, bias, first):
        scores = jnp.zeros((R, PLANE), jnp.float32)
        for p in range(PAIRS):
            dots = lax.dot_general(
                query, rows[p], (((1,), (1,)), ((), ())), preferred_element_type=jnp.float32
            )
            if dots.shape[0] == R:
                scores = jnp.where(row_pair == p, dots, scores)
            else:
                for b in range(NX):
                    mine = jnp.logical_and(row_pair == p, lane_blk == b)
                    scores = jnp.where(mine, dots[b * R : (b + 1) * R], scores)
        scores = scores * (1.0 / 8.0) + bias
        keep = -(jnp.maximum(scores, 0.0) + jnp.log1p(jnp.exp(-jnp.abs(scores))))
        pick = jnp.where(blk_i + first == blk_j, 1.0, 0.0).astype(jnp.bfloat16)
        sums = exact_dot(keep, jnp.concatenate([later, pick], axis=1))
        inside, totals = sums[:, :PLANE], sums[:, PLANE:]
        weights = jnp.exp(scores + keep + inside)
        spread = jnp.concatenate(
            [jnp.where(lane_blk == b, weights, 0.0) for b in range(NX)], axis=0
        ).astype(jnp.bfloat16)
        values = jnp.zeros((NX * R, LANES), jnp.float32)
        for p in range(PAIRS):
            out = jnp.dot(spread, rows[p], preferred_element_type=jnp.float32)
            values = jnp.where(row_pair_v == p, out, values)
        return totals, values

    q_copy.wait()
    bias_copy.wait()
    qc[...] = jnp.zeros_like(qc)
    for p in range(PAIRS):
        for g in range(GROUP):
            qc[p * GROUP + g : p * GROUP + g + 1, 0:HD] = q_v[g, p : p + 1, :]
    wide = qc[...].astype(jnp.float32)
    q_out[...] = (wide[: R // 2] + pltpu.roll(wide[R // 2 :], HD, 1)).astype(jnp.bfloat16)

    far = (z + NZ // 2) % NZ

    def query_copy(xt, slot):
        return pltpu.make_async_remote_copy(
            src_ref=q_out, dst_ref=q_in.at[slot], send_sem=qsend, recv_sem=qrecv,
            device_id={"sp": far * NX + xt}, device_id_type=MESH,
        )

    def read_copy(xt, slot):
        return pltpu.make_async_remote_copy(
            src_ref=tv_out.at[xt], dst_ref=tv_in.at[slot],
            send_sem=vsend, recv_sem=vrecv,
            device_id={"sp": far * NX + xt}, device_id_type=MESH,
        )

    def read_at_source():
        group(q_in, qsend, qrecv).wait_recv()
        rows = [stage[LAST, :, p].reshape(PLANE, LANES) for p in range(PAIRS)]
        low = lane[: R // 2] < HD
        pieces = []
        for xt in range(NX):
            wide = q_in[xt].astype(jnp.float32)
            pieces += [jnp.where(low, wide, 0.0), jnp.where(low, pltpu.roll(wide, HD, 1), 0.0)]
        query = jnp.concatenate(pieces, axis=0).astype(jnp.bfloat16)
        totals, values = read(rows, query, bias_table(lane_blk % 2 == 1), 0)
        for xt in range(NX):
            message = values[xt * R : (xt + 1) * R]
            for at, piece in enumerate(split3(totals[:, xt : xt + 1])):
                message = jnp.where(lane == at, piece.astype(jnp.float32), message)
            tv_out[xt] = message.astype(jnp.bfloat16)
        for dx in (1, 3, 2, 0):
            read_copy((xm + dx) % NX, xm).start()

    pltpu.make_async_copy(wk_hbm, wk_v, w_sem.at[0]).wait()
    pltpu.make_async_copy(wv_hbm, wv_v, w_sem.at[1]).wait()
    low_half = lax.broadcasted_iota(jnp.int32, (ROWS, LANES), 1) < HD

    def project(k, c):
        x_copy(k).wait()
        x = x_v[k].reshape(2 * ROWS, x_v.shape[-1])
        keys = jnp.dot(x, wk_v[...], preferred_element_type=jnp.float32)
        values = jnp.dot(x, wv_v[...], preferred_element_type=jnp.float32)
        for half in range(2):
            for pair in range(3):
                kk = keys[half * ROWS : (half + 1) * ROWS, pair * LANES : (pair + 1) * LANES]
                vv = values[half * ROWS : (half + 1) * ROWS, pair * LANES : (pair + 1) * LANES]
                even = jnp.where(low_half, kk, pltpu.roll(vv, HD, 1))
                odd = jnp.where(low_half, pltpu.roll(kk, HD, 1), vv)
                for side, rows in ((0, even), (1, odd)):
                    head = 2 * pair + side
                    stage[k, 2 * half + head // 3, head % 3] = rows.astype(jnp.bfloat16)

        @pl.when(k == 0)
        def _():
            pl.semaphore_wait(barrier, NSP - 1 + NTP - 1)
            for dx in range(NX):
                query_copy((xm + dx) % NX, xm).start()

        @pl.when(k == LAST)
        def _():
            read_at_source()

        @pl.when(k != LAST)
        def _():
            send_plane(k)

        return c

    lax.fori_loop(0, NZ, project, 0)

    @pl.when(tp % 2 == 0)
    def _():
        send_plane(LAST)

    for xt in range(NX):
        @pl.when(xt == xm)
        def _():
            land[:, sp] = stage[OWN, xt]

    own_bias = bias_table(sp % 2 == 1)

    def arrival(zs, k):
        return group(land.at[:, pl.ds(zs * NX, NX)], send_sem.at[k], recv_sem.at[k])

    own_group = group(land.at[:, pl.ds(0, NX - 1)], send_sem.at[OWN], recv_sem.at[OWN])

    def read_plane(at, c):
        k = at + jnp.where(at < LAST, 0, 1)
        zs = (z - plane_offset(k) + NZ) % NZ

        @pl.when(at == NZ - 2)
        def _():
            group(tv_in, vsend, vrecv).wait_recv()
            for xs in range(NX):
                message = tv_in[xs].astype(jnp.float32)
                sums = message[:, 0:1] + message[:, 1:2] + message[:, 2:3]
                tots[...] += jnp.where(lane == far * NX + xs, sums, 0.0)
                vals[far * NX + xs] = message

        @pl.when(k != OWN)
        def _():
            arrival(zs, k).wait_recv()

        @pl.when(k == OWN)
        def _():
            own_group.wait_recv()

        @pl.when(jnp.logical_and(at == NZ - 2, tp % 2 == 1))
        def _():
            send_plane(LAST)

        rows = [land[p, pl.ds(zs * NX, NX)].reshape(PLANE, LANES) for p in range(PAIRS)]
        totals, values = read(rows, qc[...], own_bias, zs * NX)
        tots[...] += totals
        for b in range(NX):
            vals[zs * NX + b] = values[b * R : (b + 1) * R]
        return c

    tots[...] = jnp.zeros((R, LANES), jnp.float32)
    lax.fori_loop(0, NZ - 1, read_plane, 0)

    def exchange(src, dst, ssem, rsem):
        return [
            pltpu.make_async_remote_copy(
                src_ref=src, dst_ref=dst.at[i], send_sem=ssem, recv_sem=rsem,
                device_id={"tp": (tp + i) % NTP}, device_id_type=MESH,
            )
            for i in range(1, NTP)
        ]

    copies = exchange(tots, tot_in, tsend, trecv)
    for copy in copies:
        copy.start()
    group(tot_in.at[pl.ds(1, NTP - 1)], tsend, trecv).wait()
    every = tots[...]
    inside_later = jnp.zeros_like(every)
    for i in range(1, NTP):
        other = tot_in[i]
        every = every + other
        inside_later = inside_later + jnp.where(tp - i < 0, other, 0.0)
    chunk_i = lax.broadcasted_iota(jnp.int32, (LANES, LANES), 0)
    chunk_j = lax.broadcasted_iota(jnp.int32, (LANES, LANES), 1)
    after = jnp.where(chunk_i > chunk_j, 1.0, 0.0).astype(jnp.bfloat16)
    scale = jnp.exp(exact_dot(every, after) + inside_later)
    partial = jnp.zeros((R, LANES), jnp.float32)
    for b in range(NSP):
        partial = partial + scale[:, b : b + 1] * vals[b]
    part[...] = partial
    copies = exchange(part, part_in, psend, precv)
    for copy in copies:
        copy.start()

    arrival(far, LAST).wait_recv()
    for k in range(NZ):
        if k == OWN:
            own_group.wait_send()
        else:
            group(stage.at[k], send_sem.at[k], recv_sem.at[k]).wait_send()
    group(q_in, qsend, qrecv).wait_send()
    group(tv_in, vsend, vrecv).wait_send()

    group(part_in.at[pl.ds(1, NTP - 1)], psend, precv).wait()
    for i in range(1, NTP):
        partial = partial + part_in[i]
    usum[...] = partial


def finish_kernel(land, usum, stored, first_read, fr_v, fr_b, out_sem, fr_sem):
    copies = [
        pltpu.make_async_copy(
            land.at[p, pl.ds(half * NSP // 4, NSP // 4)],
            stored.at[p, pl.ds(half * NSP // 4, NSP // 4)],
            out_sem.at[p, half],
        )
        for p in range(PAIRS)
        for half in range(4)
    ]
    for copy in copies:
        copy.start()
    summed = usum[...]
    lane = lax.broadcasted_iota(jnp.int32, (R, LANES), 1)
    summed = jnp.where(lane >= HD, summed, 0.0)
    squares = jnp.sum(summed * summed, axis=-1, keepdims=True) * (1.0 / HD)
    normed = summed * lax.rsqrt(squares + EPS_NORM)
    swapped = pltpu.roll(normed, HD, 1)
    for p in range(PAIRS):
        for g in range(GROUP):
            source = normed if g % 2 else swapped
            lo = (g % 2) * HD
            fr_v[p : p + 1, g * HD : (g + 1) * HD] = source[
                p * GROUP + g : p * GROUP + g + 1, lo : lo + HD
            ]
    fr_b[...] = fr_v[...].astype(jnp.bfloat16)
    fr_copy = pltpu.make_async_copy(fr_b, first_read, fr_sem.at[0])
    fr_copy.start()
    for copy in copies:
        copy.wait()
    fr_copy.wait()


def per_device(layer_input, key_weight, value_weight, queries, head_bias):
    width = layer_input.shape[-1]
    hbm = pl.BlockSpec(memory_space=pltpu.HBM)
    vmem = pl.BlockSpec(memory_space=pltpu.VMEM)
    land, usum = pl.pallas_call(
        main_kernel,
        out_shape=(
            jax.ShapeDtypeStruct((PAIRS, NSP, ROWS, LANES), jnp.bfloat16),
            jax.ShapeDtypeStruct((R, LANES), jnp.float32),
        ),
        in_specs=[hbm] * 5,
        out_specs=(vmem, vmem),
        scratch_shapes=[
            pltpu.VMEM((NZ, 2, ROWS, width), jnp.bfloat16),
            pltpu.VMEM(key_weight.shape, jnp.bfloat16),
            pltpu.VMEM(value_weight.shape, jnp.bfloat16),
            pltpu.VMEM((GROUP, PAIRS, HD), jnp.bfloat16),
            pltpu.VMEM((R, LANES), jnp.bfloat16),
            pltpu.SMEM(head_bias.shape, jnp.float32),
            pltpu.VMEM((NZ, NX, PAIRS, ROWS, LANES), jnp.bfloat16),
            pltpu.VMEM((NSP, R, LANES), jnp.float32),
            pltpu.VMEM((R, LANES), jnp.float32),
            pltpu.VMEM((R, LANES), jnp.float32),
            pltpu.VMEM((NTP, R, LANES), jnp.float32),
            pltpu.VMEM((NTP, R, LANES), jnp.float32),
            pltpu.VMEM((R // 2, LANES), jnp.bfloat16),
            pltpu.VMEM((NX, R // 2, LANES), jnp.bfloat16),
            pltpu.VMEM((NX, R, LANES), jnp.bfloat16),
            pltpu.VMEM((NX, R, LANES), jnp.bfloat16),
            pltpu.SemaphoreType.DMA((NZ,)),
            pltpu.SemaphoreType.DMA((2,)),
            pltpu.SemaphoreType.DMA((2,)),
            pltpu.SemaphoreType.DMA((NZ,)),
            pltpu.SemaphoreType.DMA((NZ,)),
            pltpu.SemaphoreType.DMA,
            pltpu.SemaphoreType.DMA,
            pltpu.SemaphoreType.DMA,
            pltpu.SemaphoreType.DMA,
            pltpu.SemaphoreType.DMA,
            pltpu.SemaphoreType.DMA,
            pltpu.SemaphoreType.DMA,
            pltpu.SemaphoreType.DMA,
        ],
        compiler_params=pltpu.CompilerParams(
            collective_id=0, has_side_effects=True, vmem_limit_bytes=40 * 1024 * 1024
        ),
        name="project_exchange_read",
    )(
        *(
            pltpu.with_memory_space_constraint(operand, pltpu.HBM)
            for operand in (
                layer_input, key_weight, value_weight, queries.transpose(1, 0, 2), head_bias
            )
        )
    )
    stored, first_read = pl.pallas_call(
        finish_kernel,
        out_shape=(
            jax.ShapeDtypeStruct(land.shape, jnp.bfloat16),
            jax.ShapeDtypeStruct((PAIRS, GROUP * HD), jnp.bfloat16),
        ),
        in_specs=[pl.BlockSpec(memory_space=pl.ANY), vmem],
        out_specs=(pl.BlockSpec(memory_space=pl.ANY), pl.BlockSpec(memory_space=pl.ANY)),
        scratch_shapes=[
            pltpu.VMEM((PAIRS, GROUP * HD), jnp.float32),
            pltpu.VMEM((PAIRS, GROUP * HD), jnp.bfloat16),
            pltpu.SemaphoreType.DMA((PAIRS, 4)),
            pltpu.SemaphoreType.DMA((1,)),
        ],
        compiler_params=pltpu.CompilerParams(vmem_limit_bytes=8 * 1024 * 1024),
        name="finish",
    )(land, usum)
    return stored, first_read


def solution(mesh):
    in_specs = (P(None, ("sp", "tp"), None), P(), P(), P("sp", None, None), P())
    out_specs = (P("sp", None, "tp", None), P("sp", None))
    return jax.shard_map(
        per_device, mesh=mesh, in_specs=in_specs, out_specs=out_specs, check_vma=False
    )
```

```python
import functools

import jax
import jax.numpy as jnp
from jax import lax
from jax.experimental import pallas as pl
from jax.experimental.pallas import tpu as pltpu
from jax.sharding import PartitionSpec as P

HD = 64
KVH = 6
GROUP = 5
EPS_NORM = 0.0001
MESH = pl.DeviceIdType.MESH

NZ = 8
NX = 4
NSP = NZ * NX
NTP = 8
PAIRS = 3
ROWS = 64
LANES = 2 * HD
R = 16
PLANE = NX * ROWS
CUTS = 4
ORDER = (1, 7, 0, 2, 6, 4, 3, 5)
OWN = ORDER.index(0)
LAST = ORDER.index(NZ // 2)


def plane_offset(k):
    offset = ORDER[-1]
    for at, value in enumerate(ORDER[:-1]):
        offset = jnp.where(k == at, value, offset)
    return offset


def split3(value):
    high = value.astype(jnp.bfloat16)
    rest = value - high.astype(jnp.float32)
    mid = rest.astype(jnp.bfloat16)
    low = (rest - mid.astype(jnp.float32)).astype(jnp.bfloat16)
    return high, mid, low


def exact_dot(value, ones):
    rows = value.shape[0]
    parts = jnp.concatenate(split3(value), axis=0)
    sums = jnp.dot(parts, ones, preferred_element_type=jnp.float32)
    return sums[:rows] + sums[rows : 2 * rows] + sums[2 * rows :]


def main_kernel(
    x_hbm, wk_hbm, wv_hbm, q_hbm, bias_hbm, land, usum,
    x_v, wk_v, wv_v, q_v, qc, bias_s, stage, vals, tots, part, tot_in, part_in,
    q_out, q_in, tv_out, tv_in,
    x_sem, w_sem, in_sem, send_sem, recv_sem, tsend, trecv, psend, precv,
    qsend, qrecv, vsend, vrecv,
):
    sp = lax.axis_index("sp")
    tp = lax.axis_index("tp")
    z = sp // NX
    xm = sp % NX

    barrier = pltpu.get_barrier_semaphore()
    for i in range(1, NSP):
        pl.semaphore_signal(
            barrier, 1, device_id={"sp": (sp + i) % NSP}, device_id_type=MESH
        )
    for i in range(1, NTP):
        pl.semaphore_signal(
            barrier, 1, device_id={"tp": (tp + i) % NTP}, device_id_type=MESH
        )

    def x_copy(k):
        zt = (z + plane_offset(k)) % NZ
        return pltpu.make_async_copy(x_hbm.at[pl.ds(2 * zt, 2)], x_v.at[k], x_sem.at[k])

    def weight_copies(w_hbm, w_v, which):
        part = w_v.shape[0] // CUTS
        return [
            pltpu.make_async_copy(
                w_hbm.at[pl.ds(i * part, part)], w_v.at[pl.ds(i * part, part)], w_sem.at[which]
            )
            for i in range(CUTS)
        ]

    weights = weight_copies(wk_hbm, wk_v, 0) + weight_copies(wv_hbm, wv_v, 1)
    q_copy = pltpu.make_async_copy(q_hbm, q_v, in_sem.at[0])
    bias_copy = pltpu.make_async_copy(bias_hbm, bias_s, in_sem.at[1])
    x_copy(0).start()
    for copy in weights:
        copy.start()
    q_copy.start()
    bias_copy.start()
    x_copy(1).start()

    def block_copy(k, xt):
        zt = (z + plane_offset(k)) % NZ
        return pltpu.make_async_remote_copy(
            src_ref=stage.at[k, xt],
            dst_ref=land.at[:, sp],
            send_sem=send_sem.at[k],
            recv_sem=recv_sem.at[k],
            device_id={"sp": zt * NX + xt},
            device_id_type=MESH,
        )

    def group(ref, ssem, rsem):
        return pltpu.make_async_remote_copy(
            src_ref=ref, dst_ref=ref, send_sem=ssem, recv_sem=rsem,
            device_id={"sp": sp}, device_id_type=MESH,
        )

    def send_plane(k):
        for dx in (1, 3, 2, 0):
            @pl.when(jnp.logical_or(k != OWN, dx != 0))
            def _():
                block_copy(k, (xm + dx) % NX).start()

    row_pair = lax.broadcasted_iota(jnp.int32, (R, PLANE), 0) // GROUP
    row_pair_v = lax.broadcasted_iota(jnp.int32, (NX * R, LANES), 0) % R // GROUP
    lane_blk = lax.broadcasted_iota(jnp.int32, (R, PLANE), 1) // ROWS
    pos_i = lax.broadcasted_iota(jnp.int32, (PLANE, PLANE), 0)
    pos_j = lax.broadcasted_iota(jnp.int32, (PLANE, PLANE), 1)
    later = jnp.logical_and(pos_i > pos_j, pos_i // ROWS == pos_j // ROWS)
    later = jnp.where(later, 1.0, 0.0).astype(jnp.bfloat16)
    blk_i = lax.broadcasted_iota(jnp.int32, (PLANE, LANES), 0) // ROWS
    blk_j = lax.broadcasted_iota(jnp.int32, (PLANE, LANES), 1)
    lane = lax.broadcasted_iota(jnp.int32, (R, LANES), 1)

    def bias_table(odd):
        row = lax.broadcasted_iota(jnp.int32, (R, PLANE), 0)
        table = jnp.zeros((R, PLANE), jnp.float32)
        for p in range(PAIRS):
            for g in range(GROUP):
                value = jnp.where(odd, bias_s[PAIRS + p, g], bias_s[p, g])
                table = jnp.where(row == p * GROUP + g, value, table)
        return table

    def read(rows, query, bias, first, with_totals=lambda totals: None):
        scores = jnp.zeros((R, PLANE), jnp.float32)
        for p in range(PAIRS):
            dots = lax.dot_general(
                query, rows[p], (((1,), (1,)), ((), ())), preferred_element_type=jnp.float32
            )
            if dots.shape[0] == R:
                scores = jnp.where(row_pair == p, dots, scores)
            else:
                for b in range(NX):
                    mine = jnp.logical_and(row_pair == p, lane_blk == b)
                    scores = jnp.where(mine, dots[b * R : (b + 1) * R], scores)
        scores = scores * (1.0 / 8.0) + bias
        keep = -(jnp.maximum(scores, 0.0) + jnp.log1p(jnp.exp(-jnp.abs(scores))))
        pick = jnp.where(blk_i + first == blk_j, 1.0, 0.0).astype(jnp.bfloat16)
        sums = exact_dot(keep, jnp.concatenate([later, pick], axis=1))
        inside, totals = sums[:, :PLANE], sums[:, PLANE:]
        with_totals(totals)
        weights = jnp.exp(scores + keep + inside)
        spread = jnp.concatenate(
            [jnp.where(lane_blk == b, weights, 0.0) for b in range(NX)], axis=0
        ).astype(jnp.bfloat16)
        values = jnp.zeros((NX * R, LANES), jnp.float32)
        for p in range(PAIRS):
            out = jnp.dot(spread, rows[p], preferred_element_type=jnp.float32)
            values = jnp.where(row_pair_v == p, out, values)
        return totals, values

    q_copy.wait()
    bias_copy.wait()
    qc[...] = jnp.zeros_like(qc)
    for p in range(PAIRS):
        for g in range(GROUP):
            qc[p * GROUP + g : p * GROUP + g + 1, 0:HD] = q_v[g, p : p + 1, :]
    wide = qc[...].astype(jnp.float32)
    q_out[...] = (wide[: R // 2] + pltpu.roll(wide[R // 2 :], HD, 1)).astype(jnp.bfloat16)

    far = (z + NZ // 2) % NZ

    def query_copy(xt, slot):
        return pltpu.make_async_remote_copy(
            src_ref=q_out, dst_ref=q_in.at[slot], send_sem=qsend, recv_sem=qrecv,
            device_id={"sp": far * NX + xt}, device_id_type=MESH,
        )

    def read_copy(xt, slot):
        return pltpu.make_async_remote_copy(
            src_ref=tv_out.at[xt], dst_ref=tv_in.at[slot],
            send_sem=vsend, recv_sem=vrecv,
            device_id={"sp": far * NX + xt}, device_id_type=MESH,
        )

    def read_at_source():
        group(q_in, qsend, qrecv).wait_recv()
        rows = [stage[LAST, :, p].reshape(PLANE, LANES) for p in range(PAIRS)]
        low = lane[: R // 2] < HD
        pieces = []
        for xt in range(NX):
            wide = q_in[xt].astype(jnp.float32)
            pieces += [jnp.where(low, wide, 0.0), jnp.where(low, pltpu.roll(wide, HD, 1), 0.0)]
        query = jnp.concatenate(pieces, axis=0).astype(jnp.bfloat16)
        totals, values = read(rows, query, bias_table(lane_blk % 2 == 1), 0)
        for xt in range(NX):
            message = values[xt * R : (xt + 1) * R]
            for at, piece in enumerate(split3(totals[:, xt : xt + 1])):
                message = jnp.where(lane == at, piece.astype(jnp.float32), message)
            tv_out[xt] = message.astype(jnp.bfloat16)
        for dx in (1, 3, 2, 0):
            read_copy((xm + dx) % NX, xm).start()

    pltpu.make_async_copy(wk_hbm, wk_v, w_sem.at[0]).wait()
    pltpu.make_async_copy(wv_hbm, wv_v, w_sem.at[1]).wait()
    for k in range(2, NZ):
        x_copy(k).start()
    low_half = lax.broadcasted_iota(jnp.int32, (ROWS, LANES), 1) < HD

    def project(k, c):
        x_copy(k).wait()
        x = x_v[k].reshape(2 * ROWS, x_v.shape[-1])
        keys = jnp.dot(x, wk_v[...], preferred_element_type=jnp.float32)
        values = jnp.dot(x, wv_v[...], preferred_element_type=jnp.float32)
        for half in range(2):
            for pair in range(3):
                kk = keys[half * ROWS : (half + 1) * ROWS, pair * LANES : (pair + 1) * LANES]
                vv = values[half * ROWS : (half + 1) * ROWS, pair * LANES : (pair + 1) * LANES]
                even = jnp.where(low_half, kk, pltpu.roll(vv, HD, 1))
                odd = jnp.where(low_half, pltpu.roll(kk, HD, 1), vv)
                for side, rows in ((0, even), (1, odd)):
                    head = 2 * pair + side
                    stage[k, 2 * half + head // 3, head % 3] = rows.astype(jnp.bfloat16)

        @pl.when(k == 0)
        def _():
            pl.semaphore_wait(barrier, NSP - 1 + NTP - 1)
            for dx in range(NX):
                query_copy((xm + dx) % NX, xm).start()

        @pl.when(k == LAST)
        def _():
            read_at_source()

        @pl.when(k != LAST)
        def _():
            send_plane(k)

        return c

    lax.fori_loop(0, NZ, project, 0)

    @pl.when(tp % 2 == 0)
    def _():
        send_plane(LAST)

    for xt in range(NX):
        @pl.when(xt == xm)
        def _():
            land[:, sp] = stage[OWN, xt]

    own_bias = bias_table(sp % 2 == 1)

    def arrival(zs, k):
        return group(land.at[:, pl.ds(zs * NX, NX)], send_sem.at[k], recv_sem.at[k])

    own_group = group(land.at[:, pl.ds(0, NX - 1)], send_sem.at[OWN], recv_sem.at[OWN])

    half = R // 2
    lane8 = lane[:half]

    def exchange(src, dst, ssem, rsem):
        for i in (4, 3, 5, 2, 6, 1, 7):
            pltpu.make_async_remote_copy(
                src_ref=src, dst_ref=dst.at[i], send_sem=ssem, recv_sem=rsem,
                device_id={"tp": (tp + i) % NTP}, device_id_type=MESH,
            ).start()

    def read_plane(at, c):
        k = at + jnp.where(at < LAST, 0, 1)
        zs = (z - plane_offset(k) + NZ) % NZ

        @pl.when(jnp.logical_and(at == NZ - 2, tp % 2 == 1))
        def _():
            send_plane(LAST)

        @pl.when(at == NZ - 2)
        def _():
            group(tv_in, vsend, vrecv).wait_recv()
            for xs in range(NX):
                message = tv_in[xs].astype(jnp.float32)
                sums = message[:, 0:1] + message[:, 1:2] + message[:, 2:3]
                sums = jnp.where(lane == far * NX + xs, sums, 0.0)
                tots[...] += sums[:half] + pltpu.roll(sums[half:], NSP, 1)
                vals[far * NX + xs] = message

        @pl.when(k != OWN)
        def _():
            arrival(zs, k).wait_recv()

        @pl.when(k == OWN)
        def _():
            own_group.wait_recv()

        rows = [land[p, pl.ds(zs * NX, NX)].reshape(PLANE, LANES) for p in range(PAIRS)]

        def add_totals(totals):
            tots[...] += totals[:half] + pltpu.roll(totals[half:], NSP, 1)

            @pl.when(at == NZ - 2)
            def _():
                exchange(tots, tot_in, tsend, trecv)

        totals, values = read(rows, qc[...], own_bias, zs * NX, add_totals)
        for b in range(NX):
            vals[zs * NX + b] = values[b * R : (b + 1) * R]
        return c

    tots[...] = jnp.zeros((half, LANES), jnp.float32)
    lax.fori_loop(0, NZ - 1, read_plane, 0)

    group(tot_in.at[pl.ds(1, NTP - 1)], tsend, trecv).wait()
    every = tots[...]
    inside_later = jnp.zeros_like(every)
    for i in range(1, NTP):
        other = tot_in[i]
        every = every + other
        inside_later = inside_later + jnp.where(tp - i < 0, other, 0.0)
    def one_below_other(packed):
        low = lane8 < NSP
        above, under = packed, pltpu.roll(packed, LANES - NSP, 1)
        return jnp.concatenate([jnp.where(low, above, 0.0), jnp.where(low, under, 0.0)], axis=0)

    every, inside_later = one_below_other(every), one_below_other(inside_later)
    chunk_i = lax.broadcasted_iota(jnp.int32, (LANES, LANES), 0)
    chunk_j = lax.broadcasted_iota(jnp.int32, (LANES, LANES), 1)
    after = jnp.where(chunk_i > chunk_j, 1.0, 0.0).astype(jnp.bfloat16)
    scale = jnp.exp(exact_dot(every, after) + inside_later)
    partial = jnp.zeros((R, LANES), jnp.float32)
    for b in range(NSP):
        partial = partial + scale[:, b : b + 1] * vals[b]
    partial = jnp.where(lane8 < HD, pltpu.roll(partial[half:], HD, 1), partial[:half])
    part[...] = partial
    exchange(part, part_in, psend, precv)

    arrival(far, LAST).wait_recv()
    for k in range(NZ):
        if k == OWN:
            own_group.wait_send()
        else:
            group(stage.at[k], send_sem.at[k], recv_sem.at[k]).wait_send()
    group(q_in, qsend, qrecv).wait_send()
    group(tv_in, vsend, vrecv).wait_send()

    group(part_in.at[pl.ds(1, NTP - 1)], psend, precv).wait()
    for i in range(1, NTP):
        partial = partial + part_in[i]
    usum[...] = jnp.concatenate([partial, pltpu.roll(partial, HD, 1)], axis=0)


def finish_kernel(land, usum, stored, first_read, fr_v, fr_b, out_sem, fr_sem):
    copies = [
        pltpu.make_async_copy(
            land.at[p, pl.ds(half * NSP // 4, NSP // 4)],
            stored.at[p, pl.ds(half * NSP // 4, NSP // 4)],
            out_sem.at[p, half],
        )
        for p in range(PAIRS)
        for half in range(4)
    ]
    for copy in copies:
        copy.start()
    summed = usum[...]
    lane = lax.broadcasted_iota(jnp.int32, (R, LANES), 1)
    summed = jnp.where(lane >= HD, summed, 0.0)
    squares = jnp.sum(summed * summed, axis=-1, keepdims=True) * (1.0 / HD)
    normed = summed * lax.rsqrt(squares + EPS_NORM)
    swapped = pltpu.roll(normed, HD, 1)
    for p in range(PAIRS):
        for g in range(GROUP):
            source = normed if g % 2 else swapped
            lo = (g % 2) * HD
            fr_v[p : p + 1, g * HD : (g + 1) * HD] = source[
                p * GROUP + g : p * GROUP + g + 1, lo : lo + HD
            ]
    fr_b[...] = fr_v[...].astype(jnp.bfloat16)
    fr_copy = pltpu.make_async_copy(fr_b, first_read, fr_sem.at[0])
    fr_copy.start()
    for copy in copies:
        copy.wait()
    fr_copy.wait()


def per_device(layer_input, key_weight, value_weight, queries, head_bias):
    width = layer_input.shape[-1]
    hbm = pl.BlockSpec(memory_space=pltpu.HBM)
    vmem = pl.BlockSpec(memory_space=pltpu.VMEM)
    land, usum = pl.pallas_call(
        main_kernel,
        out_shape=(
            jax.ShapeDtypeStruct((PAIRS, NSP, ROWS, LANES), jnp.bfloat16),
            jax.ShapeDtypeStruct((R, LANES), jnp.float32),
        ),
        in_specs=[hbm] * 5,
        out_specs=(vmem, vmem),
        scratch_shapes=[
            pltpu.VMEM((NZ, 2, ROWS, width), jnp.bfloat16),
            pltpu.VMEM(key_weight.shape, jnp.bfloat16),
            pltpu.VMEM(value_weight.shape, jnp.bfloat16),
            pltpu.VMEM((GROUP, PAIRS, HD), jnp.bfloat16),
            pltpu.VMEM((R, LANES), jnp.bfloat16),
            pltpu.SMEM(head_bias.shape, jnp.float32),
            pltpu.VMEM((NZ, NX, PAIRS, ROWS, LANES), jnp.bfloat16),
            pltpu.VMEM((NSP, R, LANES), jnp.float32),
            pltpu.VMEM((R // 2, LANES), jnp.float32),
            pltpu.VMEM((R // 2, LANES), jnp.float32),
            pltpu.VMEM((NTP, R // 2, LANES), jnp.float32),
            pltpu.VMEM((NTP, R // 2, LANES), jnp.float32),
            pltpu.VMEM((R // 2, LANES), jnp.bfloat16),
            pltpu.VMEM((NX, R // 2, LANES), jnp.bfloat16),
            pltpu.VMEM((NX, R, LANES), jnp.bfloat16),
            pltpu.VMEM((NX, R, LANES), jnp.bfloat16),
            pltpu.SemaphoreType.DMA((NZ,)),
            pltpu.SemaphoreType.DMA((2,)),
            pltpu.SemaphoreType.DMA((2,)),
            pltpu.SemaphoreType.DMA((NZ,)),
            pltpu.SemaphoreType.DMA((NZ,)),
            pltpu.SemaphoreType.DMA,
            pltpu.SemaphoreType.DMA,
            pltpu.SemaphoreType.DMA,
            pltpu.SemaphoreType.DMA,
            pltpu.SemaphoreType.DMA,
            pltpu.SemaphoreType.DMA,
            pltpu.SemaphoreType.DMA,
            pltpu.SemaphoreType.DMA,
        ],
        compiler_params=pltpu.CompilerParams(
            collective_id=0, has_side_effects=True, vmem_limit_bytes=40 * 1024 * 1024
        ),
        name="project_exchange_read",
    )(
        *(
            pltpu.with_memory_space_constraint(operand, pltpu.HBM)
            for operand in (
                layer_input, key_weight, value_weight, queries.transpose(1, 0, 2), head_bias
            )
        )
    )
    stored, first_read = pl.pallas_call(
        finish_kernel,
        out_shape=(
            jax.ShapeDtypeStruct(land.shape, jnp.bfloat16),
            jax.ShapeDtypeStruct((PAIRS, GROUP * HD), jnp.bfloat16),
        ),
        in_specs=[pl.BlockSpec(memory_space=pl.ANY), vmem],
        out_specs=(pl.BlockSpec(memory_space=pl.ANY), pl.BlockSpec(memory_space=pl.ANY)),
        scratch_shapes=[
            pltpu.VMEM((PAIRS, GROUP * HD), jnp.float32),
            pltpu.VMEM((PAIRS, GROUP * HD), jnp.bfloat16),
            pltpu.SemaphoreType.DMA((PAIRS, 4)),
            pltpu.SemaphoreType.DMA((1,)),
        ],
        compiler_params=pltpu.CompilerParams(vmem_limit_bytes=8 * 1024 * 1024),
        name="finish",
    )(land, usum)
    return stored, first_read


def solution(mesh):
    in_specs = (P(None, ("sp", "tp"), None), P(), P(), P("sp", None, None), P())
    out_specs = (P("sp", None, "tp", None), P("sp", None))
    return jax.shard_map(
        per_device, mesh=mesh, in_specs=in_specs, out_specs=out_specs, check_vma=False
    )
```

```python
import functools

import jax
import jax.numpy as jnp
from jax import lax
from jax.experimental import pallas as pl
from jax.experimental.pallas import tpu as pltpu
from jax.sharding import PartitionSpec as P

HD = 64
KVH = 6
GROUP = 5
EPS_NORM = 0.0001
MESH = pl.DeviceIdType.MESH

NZ = 8
NX = 4
NSP = NZ * NX
NTP = 8
PAIRS = 3
ROWS = 64
LANES = 2 * HD
R = 16
PLANE = NX * ROWS
CUTS = 4
ORDER = (2, 6, 0, 3, 5, 4, 1, 7)
OWN = ORDER.index(0)
LAST = ORDER.index(NZ // 2)


def plane_offset(k):
    offset = ORDER[-1]
    for at, value in enumerate(ORDER[:-1]):
        offset = jnp.where(k == at, value, offset)
    return offset


def split3(value):
    high = value.astype(jnp.bfloat16)
    rest = value - high.astype(jnp.float32)
    mid = rest.astype(jnp.bfloat16)
    low = (rest - mid.astype(jnp.float32)).astype(jnp.bfloat16)
    return high, mid, low


def exact_dot(value, ones):
    rows = value.shape[0]
    parts = jnp.concatenate(split3(value), axis=0)
    sums = jnp.dot(parts, ones, preferred_element_type=jnp.float32)
    return sums[:rows] + sums[rows : 2 * rows] + sums[2 * rows :]


def main_kernel(
    x_hbm, wk_hbm, wv_hbm, q_hbm, bias_hbm, land, usum,
    x_v, wk_v, wv_v, q_v, qc, bias_s, stage, vals, tots, part, tot_in, part_in,
    q_out, q_in, tv_out, tv_in,
    x_sem, w_sem, in_sem, send_sem, recv_sem, tsend, trecv, psend, precv,
    qsend, qrecv, vsend, vrecv,
):
    sp = lax.axis_index("sp")
    tp = lax.axis_index("tp")
    z = sp // NX
    xm = sp % NX

    def x_copy(k):
        zt = (z + plane_offset(k)) % NZ
        return pltpu.make_async_copy(x_hbm.at[pl.ds(2 * zt, 2)], x_v.at[k], x_sem.at[k])

    def weight_copies(w_hbm, w_v, which):
        part = w_v.shape[0] // CUTS
        return [
            pltpu.make_async_copy(
                w_hbm.at[pl.ds(i * part, part)], w_v.at[pl.ds(i * part, part)], w_sem.at[which]
            )
            for i in range(CUTS)
        ]

    weights = weight_copies(wk_hbm, wk_v, 0) + weight_copies(wv_hbm, wv_v, 1)
    q_copy = pltpu.make_async_copy(q_hbm, q_v, in_sem.at[0])
    bias_copy = pltpu.make_async_copy(bias_hbm, bias_s, in_sem.at[1])
    x_copy(0).start()
    for copy in weights:
        copy.start()

    barrier = pltpu.get_barrier_semaphore()
    for i in range(1, NSP):
        pl.semaphore_signal(
            barrier, 1, device_id={"sp": (sp + i) % NSP}, device_id_type=MESH
        )
    for i in range(1, NTP):
        pl.semaphore_signal(
            barrier, 1, device_id={"tp": (tp + i) % NTP}, device_id_type=MESH
        )

    q_copy.start()
    bias_copy.start()
    x_copy(1).start()

    def block_copy(k, xt):
        zt = (z + plane_offset(k)) % NZ
        return pltpu.make_async_remote_copy(
            src_ref=stage.at[k, xt],
            dst_ref=land.at[:, sp],
            send_sem=send_sem.at[k],
            recv_sem=recv_sem.at[k],
            device_id={"sp": zt * NX + xt},
            device_id_type=MESH,
        )

    def group(ref, ssem, rsem):
        return pltpu.make_async_remote_copy(
            src_ref=ref, dst_ref=ref, send_sem=ssem, recv_sem=rsem,
            device_id={"sp": sp}, device_id_type=MESH,
        )

    def send_plane(k):
        for dx in (1, 3, 2, 0):
            @pl.when(jnp.logical_or(k != OWN, dx != 0))
            def _():
                block_copy(k, (xm + dx) % NX).start()

    row_pair = lax.broadcasted_iota(jnp.int32, (R, PLANE), 0) // GROUP
    row_pair_v = lax.broadcasted_iota(jnp.int32, (NX * R, LANES), 0) % R // GROUP
    lane_blk = lax.broadcasted_iota(jnp.int32, (R, PLANE), 1) // ROWS
    pos_i = lax.broadcasted_iota(jnp.int32, (PLANE, PLANE), 0)
    pos_j = lax.broadcasted_iota(jnp.int32, (PLANE, PLANE), 1)
    later = jnp.logical_and(pos_i > pos_j, pos_i // ROWS == pos_j // ROWS)
    later = jnp.where(later, 1.0, 0.0).astype(jnp.bfloat16)
    blk_i = lax.broadcasted_iota(jnp.int32, (PLANE, LANES), 0) // ROWS
    blk_j = lax.broadcasted_iota(jnp.int32, (PLANE, LANES), 1)
    lane = lax.broadcasted_iota(jnp.int32, (R, LANES), 1)

    def bias_table(odd):
        row = lax.broadcasted_iota(jnp.int32, (R, PLANE), 0)
        table = jnp.zeros((R, PLANE), jnp.float32)
        for p in range(PAIRS):
            for g in range(GROUP):
                value = jnp.where(odd, bias_s[PAIRS + p, g], bias_s[p, g])
                table = jnp.where(row == p * GROUP + g, value, table)
        return table

    def read(rows, query, bias, first, with_totals=lambda totals: None):
        scores = jnp.zeros((R, PLANE), jnp.float32)
        for p in range(PAIRS):
            dots = lax.dot_general(
                query, rows[p], (((1,), (1,)), ((), ())), preferred_element_type=jnp.float32
            )
            if dots.shape[0] == R:
                scores = jnp.where(row_pair == p, dots, scores)
            else:
                for b in range(NX):
                    mine = jnp.logical_and(row_pair == p, lane_blk == b)
                    scores = jnp.where(mine, dots[b * R : (b + 1) * R], scores)
        scores = scores * (1.0 / 8.0) + bias
        keep = -(jnp.maximum(scores, 0.0) + jnp.log1p(jnp.exp(-jnp.abs(scores))))
        pick = jnp.where(blk_i + first == blk_j, 1.0, 0.0).astype(jnp.bfloat16)
        sums = exact_dot(keep, jnp.concatenate([later, pick], axis=1))
        inside, totals = sums[:, :PLANE], sums[:, PLANE:]
        with_totals(totals)
        weights = jnp.exp(scores + keep + inside)
        spread = jnp.concatenate(
            [jnp.where(lane_blk == b, weights, 0.0) for b in range(NX)], axis=0
        ).astype(jnp.bfloat16)
        values = jnp.zeros((NX * R, LANES), jnp.float32)
        for p in range(PAIRS):
            out = jnp.dot(spread, rows[p], preferred_element_type=jnp.float32)
            values = jnp.where(row_pair_v == p, out, values)
        return totals, values

    q_copy.wait()
    bias_copy.wait()
    qc[...] = jnp.zeros_like(qc)
    for p in range(PAIRS):
        for g in range(GROUP):
            qc[p * GROUP + g : p * GROUP + g + 1, 0:HD] = q_v[g, p : p + 1, :]
    wide = qc[...].astype(jnp.float32)
    q_out[...] = (wide[: R // 2] + pltpu.roll(wide[R // 2 :], HD, 1)).astype(jnp.bfloat16)

    far = (z + NZ // 2) % NZ

    def query_copy(xt, slot):
        return pltpu.make_async_remote_copy(
            src_ref=q_out, dst_ref=q_in.at[slot], send_sem=qsend, recv_sem=qrecv,
            device_id={"sp": far * NX + xt}, device_id_type=MESH,
        )

    def read_copy(xt, slot):
        return pltpu.make_async_remote_copy(
            src_ref=tv_out.at[xt], dst_ref=tv_in.at[slot],
            send_sem=vsend, recv_sem=vrecv,
            device_id={"sp": far * NX + xt}, device_id_type=MESH,
        )

    def read_at_source():
        group(q_in, qsend, qrecv).wait_recv()
        rows = [stage[LAST, :, p].reshape(PLANE, LANES) for p in range(PAIRS)]
        low = lane[: R // 2] < HD
        pieces = []
        for xt in range(NX):
            wide = q_in[xt].astype(jnp.float32)
            pieces += [jnp.where(low, wide, 0.0), jnp.where(low, pltpu.roll(wide, HD, 1), 0.0)]
        query = jnp.concatenate(pieces, axis=0).astype(jnp.bfloat16)
        totals, values = read(rows, query, bias_table(lane_blk % 2 == 1), 0)
        for xt in range(NX):
            message = values[xt * R : (xt + 1) * R]
            for at, piece in enumerate(split3(totals[:, xt : xt + 1])):
                message = jnp.where(lane == at, piece.astype(jnp.float32), message)
            tv_out[xt] = message.astype(jnp.bfloat16)
        for dx in (1, 3, 2, 0):
            read_copy((xm + dx) % NX, xm).start()

    pltpu.make_async_copy(wk_hbm, wk_v, w_sem.at[0]).wait()
    pltpu.make_async_copy(wv_hbm, wv_v, w_sem.at[1]).wait()
    for k in range(2, NZ):
        x_copy(k).start()
    low_half = lax.broadcasted_iota(jnp.int32, (ROWS, LANES), 1) < HD

    def project(k, c):
        x_copy(k).wait()
        x = x_v[k].reshape(2 * ROWS, x_v.shape[-1])
        keys = jnp.dot(x, wk_v[...], preferred_element_type=jnp.float32)
        values = jnp.dot(x, wv_v[...], preferred_element_type=jnp.float32)
        for half in range(2):
            for pair in range(3):
                kk = keys[half * ROWS : (half + 1) * ROWS, pair * LANES : (pair + 1) * LANES]
                vv = values[half * ROWS : (half + 1) * ROWS, pair * LANES : (pair + 1) * LANES]
                even = jnp.where(low_half, kk, pltpu.roll(vv, HD, 1))
                odd = jnp.where(low_half, pltpu.roll(kk, HD, 1), vv)
                for side, rows in ((0, even), (1, odd)):
                    head = 2 * pair + side
                    stage[k, 2 * half + head // 3, head % 3] = rows.astype(jnp.bfloat16)

        @pl.when(k == 0)
        def _():
            pl.semaphore_wait(barrier, NSP - 1 + NTP - 1)
            for dx in range(NX):
                query_copy((xm + dx) % NX, xm).start()

        @pl.when(k == LAST)
        def _():
            read_at_source()

        @pl.when(k != LAST)
        def _():
            send_plane(k)

        return c

    lax.fori_loop(0, NZ, project, 0)

    @pl.when(tp % 2 == 0)
    def _():
        send_plane(LAST)

    for xt in range(NX):
        @pl.when(xt == xm)
        def _():
            land[:, sp] = stage[OWN, xt]

    own_bias = bias_table(sp % 2 == 1)

    def arrival(zs, k):
        return group(land.at[:, pl.ds(zs * NX, NX)], send_sem.at[k], recv_sem.at[k])

    own_group = group(land.at[:, pl.ds(0, NX - 1)], send_sem.at[OWN], recv_sem.at[OWN])

    half = R // 2
    lane8 = lane[:half]

    def exchange(src, dst, ssem, rsem):
        for i in (4, 3, 5, 2, 6, 1, 7):
            pltpu.make_async_remote_copy(
                src_ref=src, dst_ref=dst.at[i], send_sem=ssem, recv_sem=rsem,
                device_id={"tp": (tp + i) % NTP}, device_id_type=MESH,
            ).start()

    def read_plane(at, c):
        k = at + jnp.where(at < LAST, 0, 1)
        zs = (z - plane_offset(k) + NZ) % NZ

        @pl.when(jnp.logical_and(at == NZ - 2, tp % 2 == 1))
        def _():
            send_plane(LAST)

        @pl.when(at == NZ - 2)
        def _():
            group(tv_in, vsend, vrecv).wait_recv()
            for xs in range(NX):
                message = tv_in[xs].astype(jnp.float32)
                sums = message[:, 0:1] + message[:, 1:2] + message[:, 2:3]
                sums = jnp.where(lane == far * NX + xs, sums, 0.0)
                tots[...] += sums[:half] + pltpu.roll(sums[half:], NSP, 1)
                vals[far * NX + xs] = message

        @pl.when(k != OWN)
        def _():
            arrival(zs, k).wait_recv()

        @pl.when(k == OWN)
        def _():
            own_group.wait_recv()

        rows = [land[p, pl.ds(zs * NX, NX)].reshape(PLANE, LANES) for p in range(PAIRS)]

        def add_totals(totals):
            tots[...] += totals[:half] + pltpu.roll(totals[half:], NSP, 1)

            @pl.when(at == NZ - 2)
            def _():
                exchange(tots, tot_in, tsend, trecv)

        totals, values = read(rows, qc[...], own_bias, zs * NX, add_totals)
        for b in range(NX):
            vals[zs * NX + b] = values[b * R : (b + 1) * R]
        return c

    tots[...] = jnp.zeros((half, LANES), jnp.float32)
    lax.fori_loop(0, NZ - 1, read_plane, 0)

    group(tot_in.at[pl.ds(1, NTP - 1)], tsend, trecv).wait()
    every = tots[...]
    inside_later = jnp.zeros_like(every)
    for i in range(1, NTP):
        other = tot_in[i]
        every = every + other
        inside_later = inside_later + jnp.where(tp - i < 0, other, 0.0)
    def one_below_other(packed):
        low = lane8 < NSP
        above, under = packed, pltpu.roll(packed, LANES - NSP, 1)
        return jnp.concatenate([jnp.where(low, above, 0.0), jnp.where(low, under, 0.0)], axis=0)

    every, inside_later = one_below_other(every), one_below_other(inside_later)
    chunk_i = lax.broadcasted_iota(jnp.int32, (LANES, LANES), 0)
    chunk_j = lax.broadcasted_iota(jnp.int32, (LANES, LANES), 1)
    after = jnp.where(chunk_i > chunk_j, 1.0, 0.0).astype(jnp.bfloat16)
    scale = jnp.exp(exact_dot(every, after) + inside_later)
    partial = jnp.zeros((R, LANES), jnp.float32)
    for b in range(NSP):
        partial = partial + scale[:, b : b + 1] * vals[b]
    partial = jnp.where(lane8 < HD, pltpu.roll(partial[half:], HD, 1), partial[:half])
    part[...] = partial
    exchange(part, part_in, psend, precv)

    arrival(far, LAST).wait_recv()
    for k in range(NZ):
        if k == OWN:
            own_group.wait_send()
        else:
            group(stage.at[k], send_sem.at[k], recv_sem.at[k]).wait_send()
    group(q_in, qsend, qrecv).wait_send()
    group(tv_in, vsend, vrecv).wait_send()

    group(part_in.at[pl.ds(1, NTP - 1)], psend, precv).wait()
    for i in range(1, NTP):
        partial = partial + part_in[i]
    usum[...] = jnp.concatenate([partial, pltpu.roll(partial, HD, 1)], axis=0)


def finish_kernel(land, usum, stored, first_read, fr_v, fr_b, out_sem, fr_sem):
    copies = [
        pltpu.make_async_copy(
            land.at[p, pl.ds(half * NSP // 4, NSP // 4)],
            stored.at[p, pl.ds(half * NSP // 4, NSP // 4)],
            out_sem.at[p, half],
        )
        for p in range(PAIRS)
        for half in range(4)
    ]
    for copy in copies:
        copy.start()
    summed = usum[...]
    lane = lax.broadcasted_iota(jnp.int32, (R, LANES), 1)
    summed = jnp.where(lane >= HD, summed, 0.0)
    squares = jnp.sum(summed * summed, axis=-1, keepdims=True) * (1.0 / HD)
    normed = summed * lax.rsqrt(squares + EPS_NORM)
    swapped = pltpu.roll(normed, HD, 1)
    for p in range(PAIRS):
        for g in range(GROUP):
            source = normed if g % 2 else swapped
            lo = (g % 2) * HD
            fr_v[p : p + 1, g * HD : (g + 1) * HD] = source[
                p * GROUP + g : p * GROUP + g + 1, lo : lo + HD
            ]
    fr_b[...] = fr_v[...].astype(jnp.bfloat16)
    fr_copy = pltpu.make_async_copy(fr_b, first_read, fr_sem.at[0])
    fr_copy.start()
    for copy in copies:
        copy.wait()
    fr_copy.wait()


def per_device(layer_input, key_weight, value_weight, queries, head_bias):
    width = layer_input.shape[-1]
    hbm = pl.BlockSpec(memory_space=pltpu.HBM)
    vmem = pl.BlockSpec(memory_space=pltpu.VMEM)
    land, usum = pl.pallas_call(
        main_kernel,
        out_shape=(
            jax.ShapeDtypeStruct((PAIRS, NSP, ROWS, LANES), jnp.bfloat16),
            jax.ShapeDtypeStruct((R, LANES), jnp.float32),
        ),
        in_specs=[hbm] * 5,
        out_specs=(vmem, vmem),
        scratch_shapes=[
            pltpu.VMEM((NZ, 2, ROWS, width), jnp.bfloat16),
            pltpu.VMEM(key_weight.shape, jnp.bfloat16),
            pltpu.VMEM(value_weight.shape, jnp.bfloat16),
            pltpu.VMEM((GROUP, PAIRS, HD), jnp.bfloat16),
            pltpu.VMEM((R, LANES), jnp.bfloat16),
            pltpu.SMEM(head_bias.shape, jnp.float32),
            pltpu.VMEM((NZ, NX, PAIRS, ROWS, LANES), jnp.bfloat16),
            pltpu.VMEM((NSP, R, LANES), jnp.float32),
            pltpu.VMEM((R // 2, LANES), jnp.float32),
            pltpu.VMEM((R // 2, LANES), jnp.float32),
            pltpu.VMEM((NTP, R // 2, LANES), jnp.float32),
            pltpu.VMEM((NTP, R // 2, LANES), jnp.float32),
            pltpu.VMEM((R // 2, LANES), jnp.bfloat16),
            pltpu.VMEM((NX, R // 2, LANES), jnp.bfloat16),
            pltpu.VMEM((NX, R, LANES), jnp.bfloat16),
            pltpu.VMEM((NX, R, LANES), jnp.bfloat16),
            pltpu.SemaphoreType.DMA((NZ,)),
            pltpu.SemaphoreType.DMA((2,)),
            pltpu.SemaphoreType.DMA((2,)),
            pltpu.SemaphoreType.DMA((NZ,)),
            pltpu.SemaphoreType.DMA((NZ,)),
            pltpu.SemaphoreType.DMA,
            pltpu.SemaphoreType.DMA,
            pltpu.SemaphoreType.DMA,
            pltpu.SemaphoreType.DMA,
            pltpu.SemaphoreType.DMA,
            pltpu.SemaphoreType.DMA,
            pltpu.SemaphoreType.DMA,
            pltpu.SemaphoreType.DMA,
        ],
        compiler_params=pltpu.CompilerParams(
            collective_id=0, has_side_effects=True, vmem_limit_bytes=40 * 1024 * 1024
        ),
        name="project_exchange_read",
    )(
        *(
            pltpu.with_memory_space_constraint(operand, pltpu.HBM)
            for operand in (
                layer_input, key_weight, value_weight, queries.transpose(1, 0, 2), head_bias
            )
        )
    )
    stored, first_read = pl.pallas_call(
        finish_kernel,
        out_shape=(
            jax.ShapeDtypeStruct(land.shape, jnp.bfloat16),
            jax.ShapeDtypeStruct((PAIRS, GROUP * HD), jnp.bfloat16),
        ),
        in_specs=[pl.BlockSpec(memory_space=pl.ANY), vmem],
        out_specs=(pl.BlockSpec(memory_space=pl.ANY), pl.BlockSpec(memory_space=pl.ANY)),
        scratch_shapes=[
            pltpu.VMEM((PAIRS, GROUP * HD), jnp.float32),
            pltpu.VMEM((PAIRS, GROUP * HD), jnp.bfloat16),
            pltpu.SemaphoreType.DMA((PAIRS, 4)),
            pltpu.SemaphoreType.DMA((1,)),
        ],
        compiler_params=pltpu.CompilerParams(vmem_limit_bytes=8 * 1024 * 1024),
        name="finish",
    )(land, usum)
    return stored, first_read


def solution(mesh):
    in_specs = (P(None, ("sp", "tp"), None), P(), P(), P("sp", None, None), P())
    out_specs = (P("sp", None, "tp", None), P("sp", None))
    return jax.shard_map(
        per_device, mesh=mesh, in_specs=in_specs, out_specs=out_specs, check_vma=False
    )
```

```python
import functools

import jax
import jax.numpy as jnp
from jax import lax
from jax.experimental import pallas as pl
from jax.experimental.pallas import tpu as pltpu
from jax.sharding import PartitionSpec as P

HD = 64
KVH = 6
GROUP = 5
EPS_NORM = 0.0001
MESH = pl.DeviceIdType.MESH

NZ = 8
NX = 4
NSP = NZ * NX
NTP = 8
PAIRS = 3
ROWS = 64
LANES = 2 * HD
R = 16
PLANE = NX * ROWS
CUTS = 4
ORDER = (2, 6, 0, 3, 5, 4, 1, 7)
OWN = ORDER.index(0)
LAST = ORDER.index(NZ // 2)


def plane_offset(k):
    offset = ORDER[-1]
    for at, value in enumerate(ORDER[:-1]):
        offset = jnp.where(k == at, value, offset)
    return offset


def split3(value):
    high = value.astype(jnp.bfloat16)
    rest = value - high.astype(jnp.float32)
    mid = rest.astype(jnp.bfloat16)
    low = (rest - mid.astype(jnp.float32)).astype(jnp.bfloat16)
    return high, mid, low


def exact_dot(value, ones):
    rows = value.shape[0]
    parts = jnp.concatenate(split3(value), axis=0)
    sums = jnp.dot(parts, ones, preferred_element_type=jnp.float32)
    return sums[:rows] + sums[rows : 2 * rows] + sums[2 * rows :]


def main_kernel(
    x_hbm, wk_hbm, wv_hbm, q_hbm, bias_hbm, land, usum,
    x_v, wk_v, wv_v, q_v, qc, bias_s, stage, vals, tots, part, tot_in, part_in,
    q_out, q_in, tv_out, tv_in,
    x_sem, w_sem, in_sem, send_sem, recv_sem, tsend, trecv, psend, precv,
    qsend, qrecv, vsend, vrecv,
):
    sp = lax.axis_index("sp")
    tp = lax.axis_index("tp")
    z = sp // NX
    xm = sp % NX

    def x_copy(k):
        zt = (z + plane_offset(k)) % NZ
        return pltpu.make_async_copy(x_hbm.at[pl.ds(2 * zt, 2)], x_v.at[k], x_sem.at[k])

    def weight_copies(w_hbm, w_v, which):
        part = w_v.shape[0] // CUTS
        return [
            pltpu.make_async_copy(
                w_hbm.at[pl.ds(i * part, part)], w_v.at[pl.ds(i * part, part)], w_sem.at[which]
            )
            for i in range(CUTS)
        ]

    weights = weight_copies(wk_hbm, wk_v, 0) + weight_copies(wv_hbm, wv_v, 1)
    q_copy = pltpu.make_async_copy(q_hbm, q_v, in_sem.at[0])
    bias_copy = pltpu.make_async_copy(bias_hbm, bias_s, in_sem.at[1])
    x_copy(0).start()
    for copy in weights:
        copy.start()

    barrier = pltpu.get_barrier_semaphore()
    for i in range(1, NSP):
        pl.semaphore_signal(
            barrier, 1, device_id={"sp": (sp + i) % NSP}, device_id_type=MESH
        )
    for i in range(1, NTP):
        pl.semaphore_signal(
            barrier, 1, device_id={"tp": (tp + i) % NTP}, device_id_type=MESH
        )

    q_copy.start()
    bias_copy.start()
    x_copy(1).start()

    def block_copy(k, xt):
        zt = (z + plane_offset(k)) % NZ
        return pltpu.make_async_remote_copy(
            src_ref=stage.at[k, xt],
            dst_ref=land.at[:, sp],
            send_sem=send_sem.at[k],
            recv_sem=recv_sem.at[k],
            device_id={"sp": zt * NX + xt},
            device_id_type=MESH,
        )

    def group(ref, ssem, rsem):
        return pltpu.make_async_remote_copy(
            src_ref=ref, dst_ref=ref, send_sem=ssem, recv_sem=rsem,
            device_id={"sp": sp}, device_id_type=MESH,
        )

    def send_plane(k):
        for dx in (1, 3, 2, 0):
            @pl.when(jnp.logical_or(k != OWN, dx != 0))
            def _():
                block_copy(k, (xm + dx) % NX).start()

    row_pair = lax.broadcasted_iota(jnp.int32, (R, PLANE), 0) // GROUP
    row_pair_v = lax.broadcasted_iota(jnp.int32, (NX * R, LANES), 0) % R // GROUP
    lane_blk = lax.broadcasted_iota(jnp.int32, (R, PLANE), 1) // ROWS
    pos_i = lax.broadcasted_iota(jnp.int32, (PLANE, PLANE), 0)
    pos_j = lax.broadcasted_iota(jnp.int32, (PLANE, PLANE), 1)
    later = jnp.logical_and(pos_i > pos_j, pos_i // ROWS == pos_j // ROWS)
    later = jnp.where(later, 1.0, 0.0).astype(jnp.bfloat16)
    blk_i = lax.broadcasted_iota(jnp.int32, (PLANE, LANES), 0) // ROWS
    blk_j = lax.broadcasted_iota(jnp.int32, (PLANE, LANES), 1)
    lane = lax.broadcasted_iota(jnp.int32, (R, LANES), 1)

    def bias_table(odd):
        row = lax.broadcasted_iota(jnp.int32, (R, PLANE), 0)
        table = jnp.zeros((R, PLANE), jnp.float32)
        for p in range(PAIRS):
            for g in range(GROUP):
                value = jnp.where(odd, bias_s[PAIRS + p, g], bias_s[p, g])
                table = jnp.where(row == p * GROUP + g, value, table)
        return table

    def read(rows, query, bias, first, with_totals=lambda totals: None):
        scores = jnp.zeros((R, PLANE), jnp.float32)
        for p in range(PAIRS):
            dots = lax.dot_general(
                query, rows[p], (((1,), (1,)), ((), ())), preferred_element_type=jnp.float32
            )
            if dots.shape[0] == R:
                scores = jnp.where(row_pair == p, dots, scores)
            else:
                for b in range(NX):
                    mine = jnp.logical_and(row_pair == p, lane_blk == b)
                    scores = jnp.where(mine, dots[b * R : (b + 1) * R], scores)
        scores = scores * (1.0 / 8.0) + bias
        keep = -(jnp.maximum(scores, 0.0) + jnp.log1p(jnp.exp(-jnp.abs(scores))))
        pick = jnp.where(blk_i + first == blk_j, 1.0, 0.0).astype(jnp.bfloat16)
        sums = exact_dot(keep, jnp.concatenate([later, pick], axis=1))
        inside, totals = sums[:, :PLANE], sums[:, PLANE:]
        with_totals(totals)
        weights = jnp.exp(scores + keep + inside)
        spread = jnp.concatenate(
            [jnp.where(lane_blk == b, weights, 0.0) for b in range(NX)], axis=0
        ).astype(jnp.bfloat16)
        values = jnp.zeros((NX * R, LANES), jnp.float32)
        for p in range(PAIRS):
            out = jnp.dot(spread, rows[p], preferred_element_type=jnp.float32)
            values = jnp.where(row_pair_v == p, out, values)
        return totals, values

    far = (z + NZ // 2) % NZ

    def query_copy(xt, slot):
        return pltpu.make_async_remote_copy(
            src_ref=q_out, dst_ref=q_in.at[slot], send_sem=qsend, recv_sem=qrecv,
            device_id={"sp": far * NX + xt}, device_id_type=MESH,
        )

    def read_copy(xt, slot):
        return pltpu.make_async_remote_copy(
            src_ref=tv_out.at[xt], dst_ref=tv_in.at[slot],
            send_sem=vsend, recv_sem=vrecv,
            device_id={"sp": far * NX + xt}, device_id_type=MESH,
        )

    def read_at_source():
        group(q_in, qsend, qrecv).wait_recv()
        rows = [stage[LAST, :, p].reshape(PLANE, LANES) for p in range(PAIRS)]
        low = lane[: R // 2] < HD
        pieces = []
        for xt in range(NX):
            wide = q_in[xt].astype(jnp.float32)
            pieces += [jnp.where(low, wide, 0.0), jnp.where(low, pltpu.roll(wide, HD, 1), 0.0)]
        query = jnp.concatenate(pieces, axis=0).astype(jnp.bfloat16)
        totals, values = read(rows, query, bias_table(lane_blk % 2 == 1), 0)
        for xt in range(NX):
            message = values[xt * R : (xt + 1) * R]
            for at, piece in enumerate(split3(totals[:, xt : xt + 1])):
                message = jnp.where(lane == at, piece.astype(jnp.float32), message)
            tv_out[xt] = message.astype(jnp.bfloat16)
        for dx in (1, 3, 2, 0):
            read_copy((xm + dx) % NX, xm).start()

    pltpu.make_async_copy(wk_hbm, wk_v, w_sem.at[0]).wait()
    low_half = lax.broadcasted_iota(jnp.int32, (ROWS, LANES), 1) < HD

    def project(k, c):
        x_copy(k).wait()
        x = x_v[k].reshape(2 * ROWS, x_v.shape[-1])
        keys = jnp.dot(x, wk_v[...], preferred_element_type=jnp.float32)

        @pl.when(k == 0)
        def _():
            pltpu.make_async_copy(wv_hbm, wv_v, w_sem.at[1]).wait()
            for other in range(2, NZ):
                x_copy(other).start()

        values = jnp.dot(x, wv_v[...], preferred_element_type=jnp.float32)
        for half in range(2):
            for pair in range(3):
                kk = keys[half * ROWS : (half + 1) * ROWS, pair * LANES : (pair + 1) * LANES]
                vv = values[half * ROWS : (half + 1) * ROWS, pair * LANES : (pair + 1) * LANES]
                even = jnp.where(low_half, kk, pltpu.roll(vv, HD, 1))
                odd = jnp.where(low_half, pltpu.roll(kk, HD, 1), vv)
                for side, rows in ((0, even), (1, odd)):
                    head = 2 * pair + side
                    stage[k, 2 * half + head // 3, head % 3] = rows.astype(jnp.bfloat16)

        @pl.when(k == 0)
        def _():
            q_copy.wait()
            bias_copy.wait()
            qc[...] = jnp.zeros_like(qc)
            for p in range(PAIRS):
                for g in range(GROUP):
                    qc[p * GROUP + g : p * GROUP + g + 1, 0:HD] = q_v[g, p : p + 1, :]
            wide = qc[...].astype(jnp.float32)
            q_out[...] = (wide[: R // 2] + pltpu.roll(wide[R // 2 :], HD, 1)).astype(jnp.bfloat16)
            pl.semaphore_wait(barrier, NSP - 1 + NTP - 1)
            for dx in range(NX):
                query_copy((xm + dx) % NX, xm).start()

        @pl.when(k == LAST)
        def _():
            read_at_source()

        @pl.when(k != LAST)
        def _():
            send_plane(k)

        return c

    lax.fori_loop(0, NZ, project, 0)

    @pl.when(tp % 2 == 0)
    def _():
        send_plane(LAST)

    for xt in range(NX):
        @pl.when(xt == xm)
        def _():
            land[:, sp] = stage[OWN, xt]

    own_bias = bias_table(sp % 2 == 1)

    def arrival(zs, k):
        return group(land.at[:, pl.ds(zs * NX, NX)], send_sem.at[k], recv_sem.at[k])

    own_group = group(land.at[:, pl.ds(0, NX - 1)], send_sem.at[OWN], recv_sem.at[OWN])

    half = R // 2
    lane8 = lane[:half]

    def exchange(src, dst, ssem, rsem):
        for i in (4, 3, 5, 2, 6, 1, 7):
            pltpu.make_async_remote_copy(
                src_ref=src, dst_ref=dst.at[i], send_sem=ssem, recv_sem=rsem,
                device_id={"tp": (tp + i) % NTP}, device_id_type=MESH,
            ).start()

    def read_plane(at, c):
        k = at + jnp.where(at < LAST, 0, 1)
        zs = (z - plane_offset(k) + NZ) % NZ

        @pl.when(jnp.logical_and(at == NZ - 2, tp % 2 == 1))
        def _():
            send_plane(LAST)

        @pl.when(at == NZ - 2)
        def _():
            group(tv_in, vsend, vrecv).wait_recv()
            for xs in range(NX):
                message = tv_in[xs].astype(jnp.float32)
                sums = message[:, 0:1] + message[:, 1:2] + message[:, 2:3]
                sums = jnp.where(lane == far * NX + xs, sums, 0.0)
                tots[...] += sums[:half] + pltpu.roll(sums[half:], NSP, 1)
                vals[far * NX + xs] = message

        @pl.when(k != OWN)
        def _():
            arrival(zs, k).wait_recv()

        @pl.when(k == OWN)
        def _():
            own_group.wait_recv()

        rows = [land[p, pl.ds(zs * NX, NX)].reshape(PLANE, LANES) for p in range(PAIRS)]

        def add_totals(totals):
            tots[...] += totals[:half] + pltpu.roll(totals[half:], NSP, 1)

            @pl.when(at == NZ - 2)
            def _():
                exchange(tots, tot_in, tsend, trecv)

        totals, values = read(rows, qc[...], own_bias, zs * NX, add_totals)
        for b in range(NX):
            vals[zs * NX + b] = values[b * R : (b + 1) * R]
        return c

    tots[...] = jnp.zeros((half, LANES), jnp.float32)
    lax.fori_loop(0, NZ - 1, read_plane, 0)

    group(tot_in.at[pl.ds(1, NTP - 1)], tsend, trecv).wait()
    every = tots[...]
    inside_later = jnp.zeros_like(every)
    for i in range(1, NTP):
        other = tot_in[i]
        every = every + other
        inside_later = inside_later + jnp.where(tp - i < 0, other, 0.0)
    def one_below_other(packed):
        low = lane8 < NSP
        above, under = packed, pltpu.roll(packed, LANES - NSP, 1)
        return jnp.concatenate([jnp.where(low, above, 0.0), jnp.where(low, under, 0.0)], axis=0)

    every, inside_later = one_below_other(every), one_below_other(inside_later)
    chunk_i = lax.broadcasted_iota(jnp.int32, (LANES, LANES), 0)
    chunk_j = lax.broadcasted_iota(jnp.int32, (LANES, LANES), 1)
    after = jnp.where(chunk_i > chunk_j, 1.0, 0.0).astype(jnp.bfloat16)
    scale = jnp.exp(exact_dot(every, after) + inside_later)
    partial = jnp.zeros((R, LANES), jnp.float32)
    for b in range(NSP):
        partial = partial + scale[:, b : b + 1] * vals[b]
    partial = jnp.where(lane8 < HD, pltpu.roll(partial[half:], HD, 1), partial[:half])
    part[...] = partial
    exchange(part, part_in, psend, precv)

    arrival(far, LAST).wait_recv()
    for k in range(NZ):
        if k == OWN:
            own_group.wait_send()
        else:
            group(stage.at[k], send_sem.at[k], recv_sem.at[k]).wait_send()
    group(q_in, qsend, qrecv).wait_send()
    group(tv_in, vsend, vrecv).wait_send()

    group(part_in.at[pl.ds(1, NTP - 1)], psend, precv).wait()
    for i in range(1, NTP):
        partial = partial + part_in[i]
    usum[...] = jnp.concatenate([partial, pltpu.roll(partial, HD, 1)], axis=0)


def finish_kernel(land, usum, stored, first_read, fr_v, fr_b, out_sem, fr_sem):
    copies = [
        pltpu.make_async_copy(
            land.at[p, pl.ds(half * NSP // 4, NSP // 4)],
            stored.at[p, pl.ds(half * NSP // 4, NSP // 4)],
            out_sem.at[p, half],
        )
        for p in range(PAIRS)
        for half in range(4)
    ]
    for copy in copies:
        copy.start()
    summed = usum[...]
    lane = lax.broadcasted_iota(jnp.int32, (R, LANES), 1)
    summed = jnp.where(lane >= HD, summed, 0.0)
    squares = jnp.sum(summed * summed, axis=-1, keepdims=True) * (1.0 / HD)
    normed = summed * lax.rsqrt(squares + EPS_NORM)
    swapped = pltpu.roll(normed, HD, 1)
    for p in range(PAIRS):
        for g in range(GROUP):
            source = normed if g % 2 else swapped
            lo = (g % 2) * HD
            fr_v[p : p + 1, g * HD : (g + 1) * HD] = source[
                p * GROUP + g : p * GROUP + g + 1, lo : lo + HD
            ]
    fr_b[...] = fr_v[...].astype(jnp.bfloat16)
    fr_copy = pltpu.make_async_copy(fr_b, first_read, fr_sem.at[0])
    fr_copy.start()
    for copy in copies:
        copy.wait()
    fr_copy.wait()


def per_device(layer_input, key_weight, value_weight, queries, head_bias):
    width = layer_input.shape[-1]
    hbm = pl.BlockSpec(memory_space=pltpu.HBM)
    vmem = pl.BlockSpec(memory_space=pltpu.VMEM)
    land, usum = pl.pallas_call(
        main_kernel,
        out_shape=(
            jax.ShapeDtypeStruct((PAIRS, NSP, ROWS, LANES), jnp.bfloat16),
            jax.ShapeDtypeStruct((R, LANES), jnp.float32),
        ),
        in_specs=[hbm] * 5,
        out_specs=(vmem, vmem),
        scratch_shapes=[
            pltpu.VMEM((NZ, 2, ROWS, width), jnp.bfloat16),
            pltpu.VMEM(key_weight.shape, jnp.bfloat16),
            pltpu.VMEM(value_weight.shape, jnp.bfloat16),
            pltpu.VMEM((GROUP, PAIRS, HD), jnp.bfloat16),
            pltpu.VMEM((R, LANES), jnp.bfloat16),
            pltpu.SMEM(head_bias.shape, jnp.float32),
            pltpu.VMEM((NZ, NX, PAIRS, ROWS, LANES), jnp.bfloat16),
            pltpu.VMEM((NSP, R, LANES), jnp.float32),
            pltpu.VMEM((R // 2, LANES), jnp.float32),
            pltpu.VMEM((R // 2, LANES), jnp.float32),
            pltpu.VMEM((NTP, R // 2, LANES), jnp.float32),
            pltpu.VMEM((NTP, R // 2, LANES), jnp.float32),
            pltpu.VMEM((R // 2, LANES), jnp.bfloat16),
            pltpu.VMEM((NX, R // 2, LANES), jnp.bfloat16),
            pltpu.VMEM((NX, R, LANES), jnp.bfloat16),
            pltpu.VMEM((NX, R, LANES), jnp.bfloat16),
            pltpu.SemaphoreType.DMA((NZ,)),
            pltpu.SemaphoreType.DMA((2,)),
            pltpu.SemaphoreType.DMA((2,)),
            pltpu.SemaphoreType.DMA((NZ,)),
            pltpu.SemaphoreType.DMA((NZ,)),
            pltpu.SemaphoreType.DMA,
            pltpu.SemaphoreType.DMA,
            pltpu.SemaphoreType.DMA,
            pltpu.SemaphoreType.DMA,
            pltpu.SemaphoreType.DMA,
            pltpu.SemaphoreType.DMA,
            pltpu.SemaphoreType.DMA,
            pltpu.SemaphoreType.DMA,
        ],
        compiler_params=pltpu.CompilerParams(
            collective_id=0, has_side_effects=True, vmem_limit_bytes=40 * 1024 * 1024
        ),
        name="project_exchange_read",
    )(
        *(
            pltpu.with_memory_space_constraint(operand, pltpu.HBM)
            for operand in (
                layer_input, key_weight, value_weight, queries.transpose(1, 0, 2), head_bias
            )
        )
    )
    stored, first_read = pl.pallas_call(
        finish_kernel,
        out_shape=(
            jax.ShapeDtypeStruct(land.shape, jnp.bfloat16),
            jax.ShapeDtypeStruct((PAIRS, GROUP * HD), jnp.bfloat16),
        ),
        in_specs=[pl.BlockSpec(memory_space=pl.ANY), vmem],
        out_specs=(pl.BlockSpec(memory_space=pl.ANY), pl.BlockSpec(memory_space=pl.ANY)),
        scratch_shapes=[
            pltpu.VMEM((PAIRS, GROUP * HD), jnp.float32),
            pltpu.VMEM((PAIRS, GROUP * HD), jnp.bfloat16),
            pltpu.SemaphoreType.DMA((PAIRS, 4)),
            pltpu.SemaphoreType.DMA((1,)),
        ],
        compiler_params=pltpu.CompilerParams(vmem_limit_bytes=8 * 1024 * 1024),
        name="finish",
    )(land, usum)
    return stored, first_read


def solution(mesh):
    in_specs = (P(None, ("sp", "tp"), None), P(), P(), P("sp", None, None), P())
    out_specs = (P("sp", None, "tp", None), P("sp", None))
    return jax.shard_map(
        per_device, mesh=mesh, in_specs=in_specs, out_specs=out_specs, check_vma=False
    )
```
